256 devices in a mesh: grp: 2 (over y), sp: 32 (over z, core), tp: 4 (over x).
Axes of the slice: x: 4, y: 2, z: 16, core: 2. Of those that a mesh axis runs over, the one named last changes fastest.
The devices are a block of a 4x16x16 slice.
Arguments:
- residual: bfloat16 [16384, 3072], P(('grp', 'sp', 'tp')), parts along dimension 0, may hold values from -3 to 3
- query_latent: bfloat16 [16384, 768], P(('grp', 'sp')), parts along dimension 0, may hold values from -6 to 6
- kv_latent: bfloat16 [16384, 384], P(('grp', 'sp')), parts along dimension 0, may hold values from -6 to 6
- rotary_key: bfloat16 [16384, 64], P(('grp', 'sp')), parts along dimension 0, may hold values from -384 to 384
- doc_ids: int32 [16384], P(('grp', 'sp')), parts along dimension 0, may hold values from 0 to 3, never falling along the last dimension, each value on 1 to 4352 neighbouring positions
- query_gain: float32 [768], replicated, may hold values from 0.1 to 1.9
- kv_gain: float32 [384], replicated, may hold values from 0.1 to 1.9
- w_query_nope: bfloat16 [768, 1536], P(None, 'tp'), may hold values from -0.625 to 0.625
- w_query_rot: bfloat16 [768, 768], P(None, 'tp'), may hold values from -0.625 to 0.625
- w_key_nope: bfloat16 [384, 1536], P(None, 'tp'), may hold values from -0.3125 to 0.3125
- w_value: bfloat16 [384, 1536], P(None, 'tp'), may hold values from -0.3125 to 0.3125
- w_out: bfloat16 [1536, 3072], P('tp'), may hold values from -0.3125 to 0.3125
- ffn_gain: float32 [3072], replicated, may hold values from 0.1 to 1.9
- w_gate: bfloat16 [32, 3072, 768], P('sp', None, 'tp'), may hold values from -0.109375 to 0.109375
- w_up: bfloat16 [32, 3072, 768], P('sp', None, 'tp'), may hold values from -0.109375 to 0.109375
- w_down: bfloat16 [32, 768, 3072], P('sp', 'tp'), may hold values from -0.4375 to 0.4375
- routes: int32 [16384, 2], P(('grp', 'sp', 'tp')), parts along dimension 0, may hold values from 0 to 31, as said below
- group_weight: float32 [16384], P(('grp', 'sp', 'tp')), parts along dimension 0, may hold values from 0.2 to 1
- member_logits: float32 [16384, 2], P(('grp', 'sp', 'tp')), parts along dimension 0, may hold values from -6 to 406
Outputs:
- layer_out: bfloat16 [16384, 3072], P(('grp', 'sp', 'tp')), parts along dimension 0
The draws below stay inside these ranges and needn't reach their ends.
There are 2 independent parts, one for each index of `grp`. The reference program is written for one: setup_inputs(seed, part) draws one part's arguments, and reference() takes and returns one part's arrays. A program takes and returns all parts, laid end to end along the dimension named above; an argument that names none is the same for every part. Nothing has to cross between parts.
Inputs may be any that keep to these rules, and one draw needn't show every extreme that they name: `routes`: the two experts of a token differ and lie in one group of 8 experts (expert e belongs to group e // 8). The 64 tokens of one device, in aligned blocks, send exactly 4 assignments to each expert. `doc_ids`: document numbers never fall along the sequence; each document has 1 to 4352 positions, one exactly 4352.
All inputs are finite; a program needn't handle non-finite values.
Results may differ from the reference program's by a relative error of at most 0.019.
The reference program's roundings to bfloat16 on the way count: a program that leaves them out, or rounds other values in their place, can miss the bound.
Values may be sent and summed in bfloat16 or wider, within the bound.
A program may use at most 128 MiB of HBM per device.

```python
import math
import jax
import jax.numpy as jnp
import numpy as np
from jax import lax

D = 3072
HEADS = 12
NOPE = 128
ROPE = 64
VDIM = 128
QL = 768
KVL = 384
FF = 768
DOCS = 4
TOKENS = 8192
ROWS_DEV = 64
EXPERTS = 32
EPG = 8
GROUPS = 4
DOC_MOST = 4352
N_TP = 4


def draw_rotary_key(key, part):
    normal_key = jax.random.fold_in(key, 0)
    drawn = jnp.clip(jax.random.normal(normal_key, (TOKENS, ROPE), jnp.float32), -6.0, 6.0)
    return drawn.astype(jnp.bfloat16)


def draw_member_logits(key, part):
    normal_key = jax.random.fold_in(key, 0)
    drawn = jnp.clip(1.5 * jax.random.normal(normal_key, (TOKENS, 2), jnp.float32), -6.0, 6.0)
    return drawn


def route_block(block_key):
    perm_key, first_key, shift_key = jax.random.split(block_key, 3)
    group_of = jax.random.permutation(perm_key, jnp.arange(ROWS_DEV, dtype=jnp.int32) % GROUPS)
    onehot = (group_of[:, None] == jnp.arange(GROUPS, dtype=jnp.int32)[None, :]).astype(jnp.int32)
    ranking = jnp.sum(onehot * (jnp.cumsum(onehot, axis=0) - 1), axis=1)
    first_off = jax.random.randint(first_key, (GROUPS,), 0, EPG)
    shift_by = jax.random.randint(shift_key, (GROUPS,), 0, EPG - 1)
    leading = (ranking + first_off[group_of]) % EPG
    trailing = (leading + 1 + shift_by[group_of]) % EPG
    return jnp.stack([group_of * EPG + leading, group_of * EPG + trailing], axis=1)


def draw_routes(key, part):
    block_keys = jax.random.split(key, TOKENS // ROWS_DEV)
    return jax.vmap(route_block)(block_keys).reshape(TOKENS, 2).astype(jnp.int32)


def steps_of(own_key, dims, shards, smallest, top_value):
    level = 1.0
    for dim, shards_of in shards:
        draws = jax.random.uniform(jax.random.fold_in(jax.random.fold_in(own_key, 6), dim), (shards_of,), jnp.float32, smallest / len(shards), top_value / len(shards))
        level = level * jnp.repeat(jnp.exp(draws), dims[dim] // shards_of).reshape((-1,) + (1,) * (len(dims) - 1 - dim))
    return level


def length_profile(amount, total, most, slope):
    loads = [(1 << 20) // math.isqrt(standing ** slope) + 1 for standing in range(2, amount + 1)]
    rest, holding = total - most - (amount - 1), [1] * (amount - 1)
    while rest > 0:
        candidates = [i for i in range(amount - 1) if holding[i] < most]
        whole, budget = sum([loads[i] for i in candidates]), rest
        for i in candidates:
            more = min(most - holding[i], max(1, budget * loads[i] // whole), rest)
            holding[i] = holding[i] + more
            rest = rest - more
    return np.array([most] + holding)


def ragged(own_key, number_of, total, most, slope):
    if number_of == 2:
        one = jax.random.randint(own_key, (), max(1, total - most), min(most, total - 1) + 1)
        return jnp.stack([one, total - one])
    lengths = jnp.asarray(length_profile(number_of, total, most, slope), jnp.int32)
    couples = (number_of - 1) // 2
    giver, taker = lengths[1:1 + 2 * couples:2], lengths[2:2 + 2 * couples:2]
    margin = jnp.minimum(giver - 1, most - taker)
    moved = jax.random.randint(jax.random.fold_in(own_key, 1), (couples,), 0, 1 << 20) % (margin + 1)
    lengths = lengths.at[1:1 + 2 * couples:2].set(giver - moved).at[2:2 + 2 * couples:2].set(taker + moved)
    return lengths[jax.random.permutation(jax.random.fold_in(own_key, 2), number_of)]


def noise(rng, shape, spread, reach, cuts=(), kind=jnp.bfloat16):
    values = spread * jax.random.normal(rng, shape, jnp.float32)
    if cuts:
        values = values * steps_of(rng, shape, cuts, -0.22, 0.18)
    return jnp.clip(values, -reach, reach).astype(kind)


def setup_inputs(seed: int = 0, part: int = 0) -> dict:
    splits = jax.random.split(jax.random.key(seed), 20)
    part_splits = jax.random.split(jax.random.fold_in(splits[19], part), 20)
    return {
        "residual": noise(part_splits[0], (TOKENS, D), 0.5, 3.0, ((0, 128),)),
        "query_latent": noise(part_splits[1], (TOKENS, QL), 1.0, 6.0, ((0, 32),)),
        "kv_latent": noise(part_splits[2], (TOKENS, KVL), 1.0, 6.0, ((0, 32),)),
        "rotary_key": draw_rotary_key(jax.random.fold_in(jax.random.fold_in(splits[19], part), 71), part),
        "doc_ids": jnp.searchsorted(jnp.cumsum(ragged(part_splits[4], DOCS, TOKENS, DOC_MOST, 0)), jnp.arange(TOKENS), side="right").astype(jnp.int32),
        "query_gain": jnp.clip(1.0 + 0.18 * jax.random.normal(splits[5], (QL,), jnp.float32), 0.1, 1.9),
        "kv_gain": jnp.clip(1.0 + 0.18 * jax.random.normal(splits[6], (KVL,), jnp.float32), 0.1, 1.9),
        "w_query_nope": noise(splits[7], (QL, HEADS * NOPE), (QL // 8) ** -0.5, 0.625, ((1, 4),)),
        "w_query_rot": noise(splits[8], (QL, HEADS * ROPE), (QL // 8) ** -0.5, 0.625, ((1, 4),)),
        "w_key_nope": noise(splits[9], (KVL, HEADS * NOPE), KVL ** -0.5, 0.3125, ((1, 4),)),
        "w_value": noise(splits[10], (KVL, HEADS * VDIM), KVL ** -0.5, 0.3125, ((1, 4),)),
        "w_out": noise(splits[11], (HEADS * VDIM, D), (HEADS * VDIM // 4) ** -0.5, 0.3125, ((0, 4),)),
        "ffn_gain": jnp.clip(1.0 + 0.18 * jax.random.normal(splits[12], (D,), jnp.float32), 0.1, 1.9),
        "w_gate": noise(splits[13], (EXPERTS, D, FF), D ** -0.5, 0.109375, ((0, 32), (2, 4))),
        "w_up": noise(splits[14], (EXPERTS, D, FF), D ** -0.5, 0.109375, ((0, 32), (2, 4))),
        "w_down": noise(splits[15], (EXPERTS, FF, D), (FF // 4) ** -0.5, 0.4375, ((0, 32), (1, 4))),
        "routes": draw_routes(jax.random.fold_in(jax.random.fold_in(splits[19], part), 71), part),
        "group_weight": jnp.clip(0.2 + 0.8 * jax.random.uniform(part_splits[17], (TOKENS,), jnp.float32) ** steps_of(part_splits[17], (TOKENS,), ((0, 128),), -0.2, 0.2), 0.2, 1.0),
        "member_logits": draw_member_logits(jax.random.fold_in(jax.random.fold_in(splits[19], part), 71), part),
    }


EPSILON = 1e-06
FLOOR_SCORE = -1e+30

def norm_rows(source, gain_vec):
    widened = source.astype(jnp.float32)
    return widened * lax.rsqrt(lax.optimization_barrier(jnp.mean(widened * widened, axis=-1, keepdims=True)) + EPSILON) * gain_vec.astype(jnp.float32)

def rotate(source, positions):
    halfway = source.shape[-1] // 2
    frequency = 10000.0 ** (-jnp.arange(halfway, dtype=jnp.float32) / halfway)
    angles = positions.astype(jnp.float32)[:, None] * frequency[None, :]
    angles = angles.reshape((source.shape[0],) + (1,) * (source.ndim - 2) + (halfway,))
    cosine = jnp.cos(angles)
    sine_part = jnp.sin(angles)
    leading = source[..., :halfway]
    trailing = source[..., halfway:]
    return jnp.concatenate([leading * cosine - trailing * sine_part, leading * sine_part + trailing * cosine], axis=-1)

def reference(residual, query_latent, kv_latent, rotary_key, doc_ids, query_gain, kv_gain, w_query_nope, w_query_rot, w_key_nope, w_value, w_out, ffn_gain, w_gate, w_up, w_down, routes, group_weight, member_logits):
    positions = jnp.arange(TOKENS, dtype=jnp.int32)
    query_normed = norm_rows(query_latent, query_gain).astype(jnp.bfloat16)
    key_normed = norm_rows(kv_latent, kv_gain).astype(jnp.bfloat16)
    query_nope = jnp.dot(query_normed, w_query_nope, preferred_element_type=jnp.float32).astype(jnp.bfloat16)
    query_nope = query_nope.reshape(TOKENS, HEADS, NOPE)
    query_rot = jnp.dot(query_normed, w_query_rot, preferred_element_type=jnp.float32).reshape(TOKENS, HEADS, ROPE)
    query_rot = rotate(query_rot, positions).astype(jnp.bfloat16)
    key_rot = rotate(rotary_key.astype(jnp.float32), positions).astype(jnp.bfloat16)
    key_nope = jnp.dot(key_normed, w_key_nope, preferred_element_type=jnp.float32).astype(jnp.bfloat16)
    values = jnp.dot(key_normed, w_value, preferred_element_type=jnp.float32).astype(jnp.bfloat16)
    key_wide = key_nope.reshape(TOKENS, HEADS, NOPE).astype(jnp.float32)
    rot_wide = key_rot.astype(jnp.float32)
    value_wide = values.reshape(TOKENS, HEADS, VDIM).astype(jnp.float32)
    factor = (NOPE + ROPE) ** (-0.5)
    block_rows = 256

    def attend(first_row):
        query_part = lax.dynamic_slice_in_dim(query_nope, first_row, block_rows, 0).astype(jnp.float32)
        rot_part = lax.dynamic_slice_in_dim(query_rot, first_row, block_rows, 0).astype(jnp.float32)
        query_pos = first_row + jnp.arange(block_rows, dtype=jnp.int32)
        query_docs = lax.dynamic_slice_in_dim(doc_ids, first_row, block_rows, 0)
        scores = jnp.einsum('qhd,khd->hqk', query_part, key_wide) + jnp.einsum('qhr,kr->hqk', rot_part, rot_wide)
        scores = scores * factor
        visible = (positions[None, :] <= query_pos[:, None]) & (doc_ids[None, :] == query_docs[:, None])
        highest = lax.optimization_barrier(jnp.max(jnp.where(visible[None], scores, FLOOR_SCORE), axis=-1, keepdims=True))
        weights = jnp.where(visible[None], jnp.exp(scores - highest), 0.0)
        totals = lax.optimization_barrier(jnp.sum(weights, axis=-1))
        rounded = lax.optimization_barrier(weights.astype(jnp.bfloat16)).astype(jnp.float32)
        summed = jnp.einsum('hqk,khd->qhd', rounded, value_wide)
        return (summed / totals.T[:, :, None]).astype(jnp.bfloat16)
    first_rows = (jnp.arange(TOKENS // block_rows) * block_rows).astype(jnp.int32)
    attended = lax.map(attend, first_rows).reshape(TOKENS, HEADS * VDIM)
    head_width = HEADS * VDIM // N_TP
    projected = jnp.zeros((TOKENS, D), jnp.float32)
    for block_index in range(N_TP):
        lower = block_index * head_width
        term = jnp.dot(attended[:, lower:lower + head_width], w_out[lower:lower + head_width], preferred_element_type=jnp.float32)
        projected = projected + lax.optimization_barrier(term.astype(jnp.bfloat16)).astype(jnp.float32)
    after_mixer = (residual.astype(jnp.float32) + projected).astype(jnp.bfloat16)
    normed = norm_rows(after_mixer, ffn_gain).astype(jnp.bfloat16)
    combine = group_weight[:, None].astype(jnp.float32) * jax.nn.softmax(member_logits.astype(jnp.float32), axis=-1)
    flat_routes = routes.reshape(-1)
    row_count = 2 * TOKENS // EXPERTS
    part_units = FF // N_TP

    def run_expert(expert):
        picked = jnp.nonzero(flat_routes == expert, size=row_count)[0].astype(jnp.int32)
        chosen = normed[picked // 2]
        gate_pre = jnp.dot(chosen, w_gate[expert], preferred_element_type=jnp.float32)
        up_pre = jnp.dot(chosen, w_up[expert], preferred_element_type=jnp.float32)
        hidden = (jax.nn.silu(gate_pre) * up_pre).astype(jnp.bfloat16)
        total = jnp.zeros((row_count, D), jnp.float32)
        for block_index in range(N_TP):
            lower = block_index * part_units
            term = jnp.dot(hidden[:, lower:lower + part_units], w_down[expert, lower:lower + part_units], preferred_element_type=jnp.float32)
            total = total + lax.optimization_barrier(term.astype(jnp.bfloat16)).astype(jnp.float32)
        return (picked, total.astype(jnp.bfloat16))
    slots, outputs = lax.map(run_expert, jnp.arange(EXPERTS, dtype=jnp.int32))
    results = jnp.zeros((2 * TOKENS, D), jnp.bfloat16).at[slots.reshape(-1)].set(outputs.reshape(-1, D))
    results = results.reshape(TOKENS, 2, D).astype(jnp.float32)
    routed_sum = lax.optimization_barrier(jnp.sum(combine[:, :, None] * results, axis=1))
    return (after_mixer.astype(jnp.float32) + routed_sum).astype(jnp.bfloat16)
```

```python
import functools

import jax
import jax.numpy as jnp
from jax import lax
from jax.experimental import pallas as pl
from jax.experimental.pallas import tpu as pltpu
from jax.sharding import PartitionSpec as P

NOPE = 128
ROPE = 64
VDIM = 128
DOC_MOST = 4352
N_DOCS = 4

EPSILON = 1e-06
FLOOR_SCORE = -1e30
MESH = pl.DeviceIdType.MESH
F32 = jnp.float32
BF16 = jnp.bfloat16


def norm_rows(source, gain_vec):
    widened = source.astype(F32)
    return (
        widened
        * lax.rsqrt(jnp.mean(widened * widened, axis=-1, keepdims=True) + EPSILON)
        * gain_vec
    )


def rotate(source, positions):
    halfway = source.shape[-1] // 2
    frequency = 10000.0 ** (-jnp.arange(halfway, dtype=F32) / halfway)
    angles = positions.astype(F32)[:, None] * frequency[None, :]
    angles = angles.reshape((source.shape[0],) + (1,) * (source.ndim - 2) + (halfway,))
    cosine = jnp.cos(angles)
    sine_part = jnp.sin(angles)
    leading = source[..., :halfway]
    trailing = source[..., halfway:]
    return jnp.concatenate(
        [leading * cosine - trailing * sine_part, leading * sine_part + trailing * cosine], axis=-1
    )


def dot(a, b):
    return jnp.dot(a, b, preferred_element_type=F32)


def attention_kernel(factor, index_ref, q_ref, kv_ref, wk_ref, wv_ref, out_ref, m_ref, l_ref, acc_ref):
    back = pl.program_id(0)
    latent_width = wk_ref.shape[0]
    heads, rows, _ = q_ref.shape

    def block(diagonal):
        latent = kv_ref[:, :latent_width]
        extra = kv_ref[:, latent_width:]
        key_nope = dot(latent, wk_ref[...]).astype(BF16)
        values = dot(latent, wv_ref[...]).astype(BF16)
        for h in range(heads):
            keys = jnp.concatenate([key_nope[:, h * NOPE : (h + 1) * NOPE], extra], axis=1)
            scores = lax.dot_general(
                q_ref[h], keys, (((1,), (1,)), ((), ())), preferred_element_type=F32
            )
            if diagonal:
                row = lax.broadcasted_iota(jnp.int32, scores.shape, 0)
                col = lax.broadcasted_iota(jnp.int32, scores.shape, 1)
                scores = jnp.where(col <= row, scores, FLOOR_SCORE)
            block_max = jnp.max(scores, axis=1, keepdims=True)
            value = values[:, h * VDIM : (h + 1) * VDIM]
            if diagonal:
                weights = jnp.exp((scores - block_max) * factor)
                m_ref[h] = block_max
                l_ref[h] = jnp.sum(weights, axis=1, keepdims=True)
                acc_ref[h] = dot(weights.astype(BF16), value)
            else:
                old = m_ref[h]
                highest = jnp.maximum(old, block_max)
                weights = jnp.exp((scores - highest) * factor)
                shrink = jnp.exp((old - highest) * factor)
                m_ref[h] = highest
                l_ref[h] = l_ref[h] * shrink + jnp.sum(weights, axis=1, keepdims=True)
                acc_ref[h] = acc_ref[h] * shrink + dot(weights.astype(BF16), value)

    @pl.when(back == 0)
    def _():
        block(True)

    @pl.when((back > 0) & (back <= index_ref[0]))
    def _():
        block(False)

    @pl.when(back == pl.num_programs(0) - 1)
    def _():
        for h in range(heads):
            out_ref[:, h * VDIM : (h + 1) * VDIM] = (acc_ref[h] / l_ref[h]).astype(out_ref.dtype)


def attention(index, queries, gathered, w_key, w_value):
    heads, rows, _ = queries.shape
    blocks = gathered.shape[0] // rows
    steps = min(blocks, 1 + (DOC_MOST + rows - 2) // rows)
    width = heads * VDIM
    return pl.pallas_call(
        functools.partial(attention_kernel, (NOPE + ROPE) ** (-0.5)),
        out_shape=jax.ShapeDtypeStruct((rows, width), BF16),
        grid_spec=pltpu.PrefetchScalarGridSpec(
            num_scalar_prefetch=1,
            grid=(steps,),
            in_specs=[
                pl.BlockSpec(queries.shape, lambda s, i: (0, 0, 0)),
                pl.BlockSpec(
                    (rows, gathered.shape[1]), lambda s, i: (lax.rem(i[0] - s + blocks, blocks), 0)
                ),
                pl.BlockSpec(w_key.shape, lambda s, i: (0, 0)),
                pl.BlockSpec(w_value.shape, lambda s, i: (0, 0)),
            ],
            out_specs=pl.BlockSpec((rows, width), lambda s, i: (0, 0)),
            scratch_shapes=[
                pltpu.VMEM((heads, rows, 1), F32),
                pltpu.VMEM((heads, rows, 1), F32),
                pltpu.VMEM((heads, rows, VDIM), F32),
            ],
        ),
        compiler_params=pltpu.CompilerParams(dimension_semantics=("arbitrary",)),
    )(index.reshape(1), queries, gathered, w_key, w_value)


COLS = 512
SPAN = 4


def offsets_of(chips):
    half, quarter = chips // 2, chips // 4
    offsets = [0, half, quarter, -quarter]
    for m in range(1, quarter):
        offsets += [m, -m, half - m, m - half]
    return offsets


def mixer_kernel(
    chips,
    att_ref, wout_ref, res_ref, gain_ref, meta_in, wg_hbm, wu_hbm, wd_hbm,
    out_ref,
    wg_ref, wu_ref, wd_ref, part, relay_l, relay_r, sum_r, sum_l, from_l, from_r, mixed,
    meta, tok, sendb, rec, back_t, back_rl, back_rr, back_sr, back_sl, back_fl, back_fr, zb, gb,
    yb, yrecv,
    wsem, pair_s, pair_r, ps, pr, zs, zr, xs, xr_, bs, br, gs, gr,
):
    sp = lax.axis_index("sp")
    x = lax.axis_index("tp")
    core = lax.rem(sp, 2)
    z = lax.div(sp, 2)
    partner = sp + 1 - 2 * core
    right, left, across = lax.rem(x + 1, 4), lax.rem(x + 3, 4), lax.rem(x + 2, 4)
    to_right, to_left, to_partner = {"tp": right}, {"tp": left}, {"sp": partner}
    offsets = offsets_of(chips)
    n_chunks = chips // SPAN
    rows, width = res_ref.shape
    half = width // 2

    def on_ring(offset):
        return {"sp": lax.rem(z + offset + chips, chips) * 2 + core}

    barrier = pltpu.get_barrier_semaphore()
    for target in [to_partner, to_left, to_right] + [on_ring(o) for o in offsets[1:]]:
        pl.semaphore_signal(barrier, inc=1, device_id=target, device_id_type=MESH)

    loads = [
        pltpu.make_async_copy(wg_hbm, wg_ref, wsem.at[0]),
        pltpu.make_async_copy(wu_hbm, wu_ref, wsem.at[1]),
        pltpu.make_async_copy(wd_hbm, wd_ref, wsem.at[2]),
    ]
    for load in loads:
        load.start()

    def remote(src, dst, ssem, rsem, target):
        return pltpu.make_async_remote_copy(
            src_ref=src, dst_ref=dst, send_sem=ssem, recv_sem=rsem, device_id=target,
            device_id_type=MESH,
        )

    def cols_of(t):
        return pl.ds(pl.multiple_of(t * COLS, COLS), COLS)

    def project(t, carry):
        value = dot(att_ref[...], wout_ref[:, cols_of(t)])
        part[:, :, cols_of(t)] = value.reshape(4, rows, COLS).astype(BF16)
        return carry

    sends = []

    def start(copy):
        copy.start()
        sends.append(copy)
        return copy

    lo, hi = pl.ds(0, half), pl.ds(half, half)
    tiles = width // COLS
    lax.fori_loop(0, tiles // 2, project, 0)
    pl.semaphore_wait(barrier, 3 + len(offsets) - 1)
    c_a = start(remote(part.at[across, :, lo], relay_l, ps.at[0], pr.at[0], to_right))
    c_d = start(remote(part.at[left, :, lo], from_r.at[:, lo], ps.at[1], pr.at[1], to_left))
    meta[core] = meta_in[...]
    m_x = start(remote(meta_in, meta.at[core], pair_s.at[0], pair_r.at[0], to_partner))
    lax.fori_loop(tiles // 2, tiles, project, 0)
    c_b = start(remote(part.at[across, :, hi], relay_r, ps.at[2], pr.at[2], to_left))
    c_c = start(remote(part.at[right, :, hi], from_l.at[:, hi], ps.at[3], pr.at[3], to_right))
    c_a.wait_recv()
    sum_r[...] = (part[right, :, :half].astype(F32) + relay_l[...].astype(F32)).astype(BF16)
    c_e = start(remote(sum_r, from_l.at[:, lo], ps.at[4], pr.at[4], to_right))
    c_b.wait_recv()
    sum_l[...] = (part[left, :, half:].astype(F32) + relay_r[...].astype(F32)).astype(BF16)
    c_f = start(remote(sum_l, from_r.at[:, hi], ps.at[5], pr.at[5], to_left))
    for copy in (c_d, c_c, c_e, c_f):
        copy.wait_recv()

    after = (
        res_ref[...].astype(F32)
        + (part[x].astype(F32) + from_l[...].astype(F32) + from_r[...].astype(F32))
    ).astype(BF16)
    mixed[...] = after
    tok[core] = norm_rows(after, gain_ref[...]).astype(BF16)
    t_x = start(remote(tok.at[core], tok.at[core], pair_s.at[1], pair_r.at[1], to_partner))
    m_x.wait_recv()
    keys = meta[...].reshape(2 * rows, meta.shape[2])
    slots = 8 * chips
    wanted = (lax.broadcasted_iota(jnp.int32, (2 * rows, slots), 1) + core * slots).astype(F32)
    first = keys[:, 0:1] == wanted
    second = keys[:, 1:2] == wanted
    choose = (first | second).astype(F32).astype(BF16)
    t_x.wait_recv()

    def select(t, carry):
        source = tok[:, :, cols_of(t)].reshape(2 * rows, COLS)
        picked = lax.dot_general(
            choose, source, (((0,), (0,)), ((), ())), preferred_element_type=F32
        )
        sendb[:, :, cols_of(t)] = picked.reshape(chips, 8, COLS).astype(BF16)
        return carry

    lax.fori_loop(0, tiles, select, 0)
    z_out = [None]
    for p in range(1, chips):
        z_out.append(
            start(
                remote(sendb.at[p], rec.at[x, p], zs.at[p], zr.at[p], on_ring(offsets[p]))
            )
        )
    rec[x, 0] = sendb[0]
    for load in loads:
        load.wait()

    fwd = [None] * n_chunks

    def spread(q):
        for p in range(q * SPAN, (q + 1) * SPAN):
            if p:
                z_out[p].wait_recv()
        whole = pl.ds(q * SPAN, SPAN)
        fwd[q] = [
            start(remote(rec.at[x, whole], rec.at[x, whole], xs.at[q, 0], xr_.at[q, 0], to_right)),
            start(remote(rec.at[x, whole], rec.at[x, whole], xs.at[q, 1], xr_.at[q, 1], to_left)),
        ]

    relays = [None] * n_chunks

    def relay(q):
        a = pl.ds(q * SPAN, SPAN // 2)
        b = pl.ds(q * SPAN + SPAN // 2, SPAN // 2)
        fwd[q][0].wait_recv()
        one = start(remote(rec.at[left, a], rec.at[left, a], xs.at[q, 2], xr_.at[q, 2], to_right))
        fwd[q][1].wait_recv()
        two = start(remote(rec.at[right, b], rec.at[right, b], xs.at[q, 3], xr_.at[q, 3], to_left))
        relays[q] = [one, two]

    backs = [None] * n_chunks
    lo2, hi2 = pl.ds(0, SPAN // 2), pl.ds(SPAN // 2, SPAN // 2)

    def experts(q):
        for copy in relays[q]:
            copy.wait_recv()
        many = 4 * SPAN * 8
        arrived = rec[:, q * SPAN : (q + 1) * SPAN].reshape(many, width)
        gate = dot(arrived, wg_ref[...])
        up = dot(arrived, wu_ref[...])
        hidden = (gate / (1.0 + jnp.exp(-gate)) * up).astype(BF16)

        def down(t, carry):
            value = dot(hidden, wd_ref[:, cols_of(t)])
            back_t[q, :, :, :, cols_of(t)] = value.reshape(4, SPAN, 8, COLS).astype(BF16)
            return carry

        lax.fori_loop(0, tiles, down, 0)
        own = back_t.at[q]
        backs[q] = [
            start(remote(own.at[across, lo2], back_rl.at[q], bs.at[q, 0], br.at[q, 0], to_right)),
            start(remote(own.at[across, hi2], back_rr.at[q], bs.at[q, 1], br.at[q, 1], to_left)),
            start(remote(own.at[right, hi2], back_fl.at[q, hi2], bs.at[q, 2], br.at[q, 2], to_right)),
            start(remote(own.at[left, lo2], back_fr.at[q, lo2], bs.at[q, 3], br.at[q, 3], to_left)),
        ]

    def add_relayed(q):
        backs[q][0].wait_recv()
        back_sr[q] = (
            back_t[q, right, : SPAN // 2].astype(F32) + back_rl[q].astype(F32)
        ).astype(BF16)
        backs[q].append(
            start(remote(back_sr.at[q], back_fl.at[q, lo2], bs.at[q, 4], br.at[q, 4], to_right))
        )
        backs[q][1].wait_recv()
        back_sl[q] = (
            back_t[q, left, SPAN // 2 :].astype(F32) + back_rr[q].astype(F32)
        ).astype(BF16)
        backs[q].append(
            start(remote(back_sl.at[q], back_fr.at[q, hi2], bs.at[q, 5], br.at[q, 5], to_left))
        )

    g_out = [None] * chips

    def give_back(q):
        for copy in backs[q][2:]:
            copy.wait_recv()
        zb[q] = (
            back_t[q, x].astype(F32) + back_fl[q].astype(F32) + back_fr[q].astype(F32)
        ).astype(BF16)
        for k in range(SPAN):
            p = q * SPAN + k
            if p:
                g_out[p] = start(
                    remote(zb.at[q, k], gb.at[p], gs.at[p], gr.at[p], on_ring(-offsets[p]))
                )
            else:
                gb[0] = zb[0, 0]

    stages = (spread, relay, experts, add_relayed, give_back)
    for tick in range(n_chunks + len(stages) - 1):
        for s in reversed(range(len(stages))):
            if 0 <= tick - s < n_chunks:
                stages[s](tick - s)

    for p in range(1, chips):
        g_out[p].wait_recv()
    weigh = jnp.where(first, keys[:, 2:3], 0.0) + jnp.where(second, keys[:, 3:4], 0.0)
    weigh_hi = weigh.astype(BF16)
    weigh_lo = (weigh - weigh_hi.astype(F32)).astype(BF16)

    def combine(t, carry):
        returned = gb[:, :, cols_of(t)].reshape(slots, COLS)
        yb[:, :, cols_of(t)] = (dot(weigh_hi, returned) + dot(weigh_lo, returned)).reshape(
            2, rows, COLS
        )
        return carry

    lax.fori_loop(0, tiles, combine, 0)
    y_x = start(remote(yb.at[1 - core], yrecv, pair_s.at[2], pair_r.at[2], to_partner))
    y_x.wait_recv()
    out_ref[...] = (mixed[...].astype(F32) + (yb[core] + yrecv[...])).astype(out_ref.dtype)
    for copy in sends:
        copy.wait_send()


def mixer(attended, w_out, residual, gain, meta, w_gate, w_up, w_down, chips):
    rows, width = residual.shape
    n_chunks = chips // SPAN
    vmem = pl.BlockSpec(memory_space=pltpu.VMEM)
    hbm = pl.BlockSpec(memory_space=pl.ANY)
    half = width // 2
    dma = pltpu.SemaphoreType.DMA
    chunk = (n_chunks, SPAN, 8, width)
    half_chunk = (n_chunks, SPAN // 2, 8, width)
    return pl.pallas_call(
        functools.partial(mixer_kernel, chips),
        out_shape=jax.ShapeDtypeStruct((rows, width), BF16),
        in_specs=[vmem] * 5 + [hbm] * 3,
        out_specs=vmem,
        scratch_shapes=[
            pltpu.VMEM(w_gate.shape, BF16),
            pltpu.VMEM(w_up.shape, BF16),
            pltpu.VMEM(w_down.shape, BF16),
            pltpu.VMEM((4, rows, width), BF16),
            pltpu.VMEM((rows, half), BF16),
            pltpu.VMEM((rows, half), BF16),
            pltpu.VMEM((rows, half), BF16),
            pltpu.VMEM((rows, half), BF16),
            pltpu.VMEM((rows, width), BF16),
            pltpu.VMEM((rows, width), BF16),
            pltpu.VMEM((rows, width), BF16),
            pltpu.VMEM((2, rows, meta.shape[1]), F32),
            pltpu.VMEM((2, rows, width), BF16),
            pltpu.VMEM((chips, 8, width), BF16),
            pltpu.VMEM((4, chips, 8, width), BF16),
            pltpu.VMEM((n_chunks, 4, SPAN, 8, width), BF16),
            pltpu.VMEM(half_chunk, BF16),
            pltpu.VMEM(half_chunk, BF16),
            pltpu.VMEM(half_chunk, BF16),
            pltpu.VMEM(half_chunk, BF16),
            pltpu.VMEM(chunk, BF16),
            pltpu.VMEM(chunk, BF16),
            pltpu.VMEM(chunk, BF16),
            pltpu.VMEM((chips, 8, width), BF16),
            pltpu.VMEM((2, rows, width), F32),
            pltpu.VMEM((rows, width), F32),
            dma((3,)),
            dma((3,)),
            dma((3,)),
            dma((6,)),
            dma((6,)),
            dma((chips,)),
            dma((chips,)),
            dma((n_chunks, 4)),
            dma((n_chunks, 4)),
            dma((n_chunks, 6)),
            dma((n_chunks, 6)),
            dma((chips,)),
            dma((chips,)),
        ],
        compiler_params=pltpu.CompilerParams(
            collective_id=0, has_side_effects=True, vmem_limit_bytes=56 * 1024 * 1024
        ),
    )(attended, w_out, residual, gain, meta, w_gate, w_up, w_down)


def routing_meta(routes, group_weight, member_logits, chips):
    sp = lax.axis_index("sp")
    core, z = sp % 2, sp // 2
    flat = routes.reshape(-1)
    count = flat.shape[0]
    earlier = jnp.arange(count)[None, :] < jnp.arange(count)[:, None]
    same = flat[:, None] == flat[None, :]
    ranking = jnp.sum((same & earlier).astype(jnp.int32), axis=1).reshape(routes.shape)
    distance = (routes // 2 - z + chips) % chips
    position = jnp.zeros_like(routes)
    for p, offset in enumerate(offsets_of(chips)):
        position = jnp.where(distance == offset % chips, p, position)
    key = (routes % 2) * (8 * chips) + position * 8 + core * 4 + ranking
    weights = group_weight[:, None] * jax.nn.softmax(member_logits, axis=-1)
    filler = jnp.zeros((routes.shape[0], 124), F32)
    return jnp.concatenate([key.astype(F32), weights, filler], axis=1)


def on_device(
    residual,
    query_latent,
    kv_latent,
    rotary_key,
    doc_ids,
    query_gain,
    kv_gain,
    w_query_nope,
    w_query_rot,
    w_key_nope,
    w_value,
    w_out,
    ffn_gain,
    w_gate,
    w_up,
    w_down,
    routes,
    group_weight,
    member_logits,
):
    queries_here = query_latent.shape[0]
    heads_here = w_key_nope.shape[1] // NOPE
    index = lax.axis_index("sp")
    chips = lax.axis_size("sp") // 2
    query_pos = index * queries_here + jnp.arange(queries_here, dtype=jnp.int32)
    is_doc = doc_ids[:, None] == jnp.arange(ROPE, dtype=jnp.int32)[None, :]
    key_normed = norm_rows(kv_latent, kv_gain).astype(BF16)
    key_rot = rotate(rotary_key.astype(F32), query_pos).astype(BF16)
    own = jnp.concatenate([key_normed, key_rot, is_doc.astype(BF16)], axis=1)
    gathered = lax.all_gather(own, "sp", axis=0, tiled=True)

    query_normed = norm_rows(query_latent, query_gain).astype(BF16)
    query_nope = dot(query_normed, w_query_nope).astype(BF16)
    query_nope = query_nope.reshape(queries_here, heads_here, NOPE)
    query_rot = dot(query_normed, w_query_rot).reshape(queries_here, heads_here, ROPE)
    query_rot = rotate(query_rot, query_pos).astype(BF16)
    other_doc = jnp.where(is_doc, 0.0, FLOOR_SCORE).astype(BF16)
    other_doc = jnp.broadcast_to(other_doc[:, None, :], query_rot.shape)
    queries = jnp.concatenate([query_nope, query_rot, other_doc], axis=2).transpose(1, 0, 2)

    attended = attention(index, queries, gathered, w_key_nope, w_value)
    meta = routing_meta(routes, group_weight, member_logits, chips)
    return mixer(
        attended, w_out, residual, ffn_gain[None, :], meta, w_gate[0], w_up[0], w_down[0], chips
    )


def solution(mesh):
    return jax.shard_map(
        on_device,
        mesh=mesh,
        in_specs=(
            P(("grp", "sp", "tp"), None),
            P(("grp", "sp"), None),
            P(("grp", "sp"), None),
            P(("grp", "sp"), None),
            P(("grp", "sp")),
            P(),
            P(),
            P(None, "tp"),
            P(None, "tp"),
            P(None, "tp"),
            P(None, "tp"),
            P("tp", None),
            P(),
            P("sp", None, "tp"),
            P("sp", None, "tp"),
            P("sp", "tp", None),
            P(("grp", "sp", "tp"), None),
            P(("grp", "sp", "tp")),
            P(("grp", "sp", "tp"), None),
        ),
        out_specs=P(("grp", "sp", "tp"), None),
        check_vma=False,
    )
```

```python
import functools
import math

import jax
import jax.numpy as jnp
from jax import lax
from jax.experimental import pallas as pl
from jax.experimental.pallas import tpu as pltpu
from jax.sharding import PartitionSpec as P

NOPE = 128
ROPE = 64
VDIM = 128
DOC_MOST = 4352

EPSILON = 1e-06
FLOOR_SCORE = -1e30
MESH = pl.DeviceIdType.MESH
F32 = jnp.float32
BF16 = jnp.bfloat16


def norm_rows(source, gain_vec):
    widened = source.astype(F32)
    return (
        widened
        * lax.rsqrt(jnp.mean(widened * widened, axis=-1, keepdims=True) + EPSILON)
        * gain_vec
    )


def dot(a, b):
    return jnp.dot(a, b, preferred_element_type=F32)


def dot_nt(a, b):
    return lax.dot_general(a, b, (((1,), (1,)), ((), ())), preferred_element_type=F32)


def attention_kernel(
    factor, hops, seed,
    ql_ref, kl_ref, rk_ref, doc_ref, qg_ref, kg_ref, wqn_ref, wqr_ref, wk_ref, wv_ref,
    out_ref,
    kv, keys_ref, values_ref, q_ref, m_ref, l_ref, acc_ref, zs, zr, xs, xr_, ds, dr,
):
    sp = lax.axis_index("sp")
    n_sp = lax.axis_size("sp")
    x = lax.axis_index("tp")
    core = lax.rem(sp, 2)
    z = lax.div(sp, 2)
    right, left, across = lax.rem(x + 1, 4), lax.rem(x + 3, 4), lax.rem(x + 2, 4)
    to_right, to_left, to_partner = {"tp": right}, {"tp": left}, {"sp": sp + 1 - 2 * core}

    def chip_at(offset):
        return {"sp": lax.rem(sp + 2 * offset + n_sp, n_sp)}

    rows = ql_ref.shape[0]
    heads = q_ref.shape[0]
    latent_width = wk_ref.shape[0]
    quarter = rows // 4

    barrier = pltpu.get_barrier_semaphore()
    greeted = [to_partner, to_left, to_right] + [chip_at(o) for o in (1, -1, seed, -seed)]
    for target in greeted:
        pl.semaphore_signal(barrier, inc=1, device_id=target, device_id_type=MESH)

    def remote(src, dst, ssem, rsem, target):
        return pltpu.make_async_remote_copy(
            src_ref=src, dst_ref=dst, send_sem=ssem, recv_sem=rsem, device_id=target,
            device_id_type=MESH,
        )

    def onward(h):
        return remote(
            kv.at[h, core, x], kv.at[h + 1, core, x], zs.at[h + 1], zr.at[h + 1], chip_at(1)
        )

    def jump():
        return remote(
            kv.at[0, core, x], kv.at[seed, core, x], zs.at[seed], zr.at[seed], chip_at(seed)
        )

    def beside(h, k):
        owner = (x, x, left, right)[k]
        target = (to_right, to_left, to_right, to_left)[k]
        part = kv.at[h, core, owner]
        if k >= 2:
            part = part.at[pl.ds((k - 2) * (quarter // 2), quarter // 2)]
        return remote(part, part, xs.at[h, k], xr_.at[h, k], target)

    def shared(h):
        return [
            remote(
                r.at[h, core], r.at[h, core], ds.at[h, k], dr.at[h, k], to_partner
            )
            for k, r in enumerate((keys_ref, values_ref))
        ]

    step = -math.log(10000.0) / (ROPE // 2)
    frequency = jnp.exp(
        lax.broadcasted_iota(jnp.int32, (ROPE // 2, rows), 0).astype(F32) * step
    )
    position = (sp * rows + lax.broadcasted_iota(jnp.int32, (ROPE // 2, rows), 1)).astype(F32)
    angles = position * frequency
    cosine, sine = jnp.cos(angles), jnp.sin(angles)

    def turned(source):
        a, b = source[: ROPE // 2], source[ROPE // 2 :]
        return jnp.concatenate([a * cosine - b * sine, a * sine + b * cosine], axis=0)

    docs = jnp.broadcast_to(doc_ref[...], (ROPE, rows))
    same_doc = docs == lax.broadcasted_iota(jnp.int32, (ROPE, rows), 0)
    key_tail = jnp.concatenate(
        [turned(rk_ref[...].astype(F32)), same_doc.astype(F32)], axis=0
    ).T.astype(BF16)
    latent = norm_rows(kl_ref[...], kg_ref[...][None, :]).astype(BF16)
    own = jnp.concatenate([latent, key_tail], axis=1)
    kv[0, core] = own.reshape(4, quarter, own.shape[1])
    pl.semaphore_wait(barrier, len(greeted))
    onward(0).start()
    jump().start()

    def project(h):
        block = kv[h, core].reshape(rows, kv.shape[-1])
        latent = block[:, :latent_width]
        keys_ref[h, core, :, :latent_width] = dot(latent, wk_ref[...]).astype(BF16)
        keys_ref[h, core, :, latent_width:] = block[:, latent_width:]
        values_ref[h, core] = lax.dot_general(
            wv_ref[...], latent, (((0,), (1,)), ((), ())), preferred_element_type=F32
        ).astype(BF16)
        for copy in shared(h):
            copy.start()

    project(0)

    query_normed = norm_rows(ql_ref[...], qg_ref[...][None, :]).astype(BF16)
    nope = lax.dot_general(
        wqn_ref[...], query_normed, (((0,), (1,)), ((), ())), preferred_element_type=F32
    )
    rot = dot_nt(wqr_ref[...], query_normed)
    reject = jnp.where(same_doc, 0.0, FLOOR_SCORE)
    for h in range(heads):
        q_ref[h] = jnp.concatenate(
            [nope[h * NOPE : (h + 1) * NOPE], turned(rot[h * ROPE : (h + 1) * ROPE]), reject],
            axis=0,
        ).astype(BF16)

    def attend(h, blocks, diagonal):
        scores, values = [], []
        for b in blocks:
            keys = keys_ref[h, b]
            tail = keys[:, latent_width:]
            values.append(values_ref[h, b])
            scores.append([
                dot(
                    jnp.concatenate([keys[:, i * NOPE : (i + 1) * NOPE], tail], axis=1), q_ref[i]
                )
                for i in range(heads)
            ])
        if diagonal:
            shape = (rows, rows)
            col = core * rows + lax.broadcasted_iota(jnp.int32, shape, 1)
            row = lax.broadcasted_iota(jnp.int32, shape, 0)
            scores = [
                [jnp.where(row + k * rows <= col, s, FLOOR_SCORE) for s in block]
                for k, block in enumerate(scores)
            ]
        for i in range(heads):
            mine = [block[i] for block in scores]
            highest = functools.reduce(
                jnp.maximum, [jnp.max(s, axis=0, keepdims=True) for s in mine]
            )
            if not diagonal:
                old = m_ref[i]
                highest = jnp.maximum(old, highest)
            weights = [jnp.exp((s - highest) * factor) for s in mine]
            total = sum(jnp.sum(w, axis=0, keepdims=True) for w in weights)
            attended = sum(
                dot(v[i * VDIM : (i + 1) * VDIM], w.astype(BF16)) for v, w in zip(values, weights)
            )
            if not diagonal:
                shrink = jnp.exp((old - highest) * factor)
                total = l_ref[i] * shrink + total
                attended = acc_ref[i] * shrink + attended
            m_ref[i] = highest
            l_ref[i] = total
            acc_ref[i] = attended

    def hop_at(n):
        return jnp.where(n == hops, n, jnp.where(n % 2 == 1, (n + 1) // 2, seed - 1 + n // 2))

    def held(n):
        return (n >= 1) & ((n < hops) | ((n == hops) & (core == 1)))

    def goes_on(h):
        return (h != seed - 1) & ((h < hops - 1) | ((h == hops - 1) & (core == 1)))

    def arrive(n):
        @pl.when(held(n))
        def _():
            h = hop_at(n)
            onward(h - 1).wait_recv()

            @pl.when(goes_on(h))
            def _():
                onward(h).start()

            beside(h, 0).start()
            beside(h, 1).start()

    def pass_on(n):
        @pl.when(held(n))
        def _():
            h = hop_at(n)
            beside(h, 0).wait_recv()
            beside(h, 2).start()
            beside(h, 1).wait_recv()
            beside(h, 3).start()

    def share(n):
        @pl.when(held(n))
        def _():
            h = hop_at(n)
            beside(h, 2).wait_recv()
            beside(h, 3).wait_recv()
            project(h)

    def use(n):
        @pl.when((n >= 1) & (n < hops))
        def _():
            h = hop_at(n)
            for copy in shared(h):
                copy.wait_recv()

            @pl.when(h <= z)
            def _():
                attend(h, (0, 1), False)

    arrive(1)
    for copy in shared(0):
        copy.wait_recv()
    attend(0, (0, 1), True)

    def tick(t, carry):
        arrive(t)
        pass_on(t - 1)
        share(t - 2)
        use(t - 3)
        return carry

    lax.fori_loop(2, hops + 3, tick, 0)

    @pl.when(core == 0)
    def _():
        for copy in shared(hops):
            copy.wait_recv()

        @pl.when(hops <= z)
        def _():
            attend(hops, (1,), False)

    for i in range(heads):
        out_ref[:, i * VDIM : (i + 1) * VDIM] = (acc_ref[i] / l_ref[i]).T.astype(out_ref.dtype)

    onward(0).wait_send()
    jump().wait_send()
    for copy in shared(0):
        copy.wait_send()

    def drain(h, carry):
        @pl.when(held(h))
        def _():
            @pl.when(goes_on(h))
            def _():
                onward(h).wait_send()

            for k in range(4):
                beside(h, k).wait_send()
            for copy in shared(h):
                copy.wait_send()

        return carry

    lax.fori_loop(1, hops + 1, drain, 0)


def attention(
    query_latent, kv_latent, rotary_key, doc_ids, query_gain, kv_gain, w_query_nope, w_query_rot,
    w_key, w_value,
):
    rows = query_latent.shape[0]
    heads = w_key.shape[1] // NOPE
    width = heads * VDIM
    latent_width = kv_latent.shape[1]
    blocks_back = (DOC_MOST + rows - 2) // rows
    hops = (blocks_back + 1) // 2
    assert blocks_back % 2 == 1 and hops % 2 == 1
    seed = (hops + 1) // 2
    vmem = pl.BlockSpec(memory_space=pltpu.VMEM)
    dma = pltpu.SemaphoreType.DMA
    return pl.pallas_call(
        functools.partial(attention_kernel, (NOPE + ROPE) ** (-0.5), hops, seed),
        out_shape=jax.ShapeDtypeStruct((rows, width), BF16),
        in_specs=[vmem] * 10,
        out_specs=vmem,
        scratch_shapes=[
            pltpu.VMEM((hops + 1, 2, 4, rows // 4, latent_width + 2 * ROPE), BF16),
            pltpu.VMEM((hops + 1, 2, rows, width + 2 * ROPE), BF16),
            pltpu.VMEM((hops + 1, 2, width, rows), BF16),
            pltpu.VMEM((heads, 2 * NOPE, rows), BF16),
            pltpu.VMEM((heads, 1, rows), F32),
            pltpu.VMEM((heads, 1, rows), F32),
            pltpu.VMEM((heads, VDIM, rows), F32),
            dma((hops + 1,)),
            dma((hops + 1,)),
            dma((hops + 1, 4)),
            dma((hops + 1, 4)),
            dma((hops + 1, 2)),
            dma((hops + 1, 2)),
        ],
        compiler_params=pltpu.CompilerParams(
            collective_id=1, has_side_effects=True, vmem_limit_bytes=56 * 1024 * 1024
        ),
    )(
        query_latent, kv_latent, rotary_key.T, doc_ids[None, :],
        query_gain, kv_gain, w_query_nope, w_query_rot.T, w_key, w_value,
    )


COLS = 512
SPAN = 4


def offsets_of(chips):
    half, quarter = chips // 2, chips // 4
    offsets = [0, half, quarter, -quarter]
    for m in range(1, quarter):
        offsets += [m, -m, half - m, m - half]
    return offsets


def mixer_kernel(
    chips,
    att_ref, wout_ref, res_ref, gain_ref, routes_ref, group_ref, logits_ref, wg_hbm, wu_hbm, wd_hbm,
    out_ref,
    wg_ref, wu_ref, wd_ref, part, relay_l, relay_r, sum_r, sum_l, from_l, from_r, mixed,
    meta, tok, sendb, rec, back_t, back_rl, back_rr, back_sr, back_sl, back_fl, back_fr, zb, gb,
    yb, yrecv,
    wsem, pair_s, pair_r, ps, pr, zs, zr, xs, xr_, bs, br, gs, gr,
):
    sp = lax.axis_index("sp")
    x = lax.axis_index("tp")
    core = lax.rem(sp, 2)
    z = lax.div(sp, 2)
    partner = sp + 1 - 2 * core
    right, left, across = lax.rem(x + 1, 4), lax.rem(x + 3, 4), lax.rem(x + 2, 4)
    to_right, to_left, to_partner = {"tp": right}, {"tp": left}, {"sp": partner}
    offsets = offsets_of(chips)
    n_chunks = chips // SPAN
    rows, width = res_ref.shape
    half = width // 2

    def on_ring(offset):
        return {"sp": lax.rem(z + offset + chips, chips) * 2 + core}

    barrier = pltpu.get_barrier_semaphore()
    for target in [to_partner, to_left, to_right] + [on_ring(o) for o in offsets[1:]]:
        pl.semaphore_signal(barrier, inc=1, device_id=target, device_id_type=MESH)

    loads = [
        pltpu.make_async_copy(wg_hbm, wg_ref, wsem.at[0]),
        pltpu.make_async_copy(wu_hbm, wu_ref, wsem.at[1]),
        pltpu.make_async_copy(wd_hbm, wd_ref, wsem.at[2]),
    ]
    for load in loads:
        load.start()

    def remote(src, dst, ssem, rsem, target):
        return pltpu.make_async_remote_copy(
            src_ref=src, dst_ref=dst, send_sem=ssem, recv_sem=rsem, device_id=target,
            device_id_type=MESH,
        )

    def cols_of(t):
        return pl.ds(pl.multiple_of(t * COLS, COLS), COLS)

    routes = routes_ref[...]
    expert = lax.broadcasted_iota(jnp.int32, (2 * chips, rows), 0)
    goes = [routes[k : k + 1] == expert for k in range(2)]
    earlier = (
        lax.broadcasted_iota(jnp.int32, (rows, rows), 0)
        < lax.broadcasted_iota(jnp.int32, (rows, rows), 1)
    )
    before = dot(
        (goes[0] | goes[1]).astype(F32).astype(BF16), earlier.astype(F32).astype(BF16)
    )
    distance = lax.rem(lax.div(routes, 2) - z + chips, chips)
    place = jnp.zeros_like(routes)
    for p, offset in enumerate(offsets):
        place = jnp.where(distance == offset % chips, p, place)
    spot = (lax.rem(routes, 2) * (8 * chips) + place * 8 + core * 4).astype(F32)
    ranks = [jnp.sum(jnp.where(g, before, 0.0), axis=0, keepdims=True) for g in goes]
    logits = logits_ref[...]
    top = jnp.maximum(logits[0:1], logits[1:2])
    powers = [jnp.exp(logits[k : k + 1] - top) for k in range(2)]
    share = group_ref[...][None, :] / (powers[0] + powers[1])
    table = [spot[k : k + 1] + ranks[k] for k in range(2)] + [p * share for p in powers]
    table.append(jnp.zeros((meta.shape[2] - 4, rows), F32))
    meta[core] = jnp.concatenate(table, axis=0).T

    def project(t, carry):
        value = dot(att_ref[...], wout_ref[:, cols_of(t)])
        part[:, :, cols_of(t)] = value.reshape(4, rows, COLS).astype(BF16)
        return carry

    sends = []

    def start(copy):
        copy.start()
        sends.append(copy)
        return copy

    lo, hi = pl.ds(0, half), pl.ds(half, half)
    tiles = width // COLS
    lax.fori_loop(0, tiles // 2, project, 0)
    pl.semaphore_wait(barrier, 3 + len(offsets) - 1)
    c_a = start(remote(part.at[across, :, lo], relay_l, ps.at[0], pr.at[0], to_right))
    c_d = start(remote(part.at[left, :, lo], from_r.at[:, lo], ps.at[1], pr.at[1], to_left))
    m_x = start(remote(meta.at[core], meta.at[core], pair_s.at[0], pair_r.at[0], to_partner))
    lax.fori_loop(tiles // 2, tiles, project, 0)
    c_b = start(remote(part.at[across, :, hi], relay_r, ps.at[2], pr.at[2], to_left))
    c_c = start(remote(part.at[right, :, hi], from_l.at[:, hi], ps.at[3], pr.at[3], to_right))
    c_a.wait_recv()
    sum_r[...] = (part[right, :, :half].astype(F32) + relay_l[...].astype(F32)).astype(BF16)
    c_e = start(remote(sum_r, from_l.at[:, lo], ps.at[4], pr.at[4], to_right))
    c_b.wait_recv()
    sum_l[...] = (part[left, :, half:].astype(F32) + relay_r[...].astype(F32)).astype(BF16)
    c_f = start(remote(sum_l, from_r.at[:, hi], ps.at[5], pr.at[5], to_left))
    for copy in (c_d, c_c, c_e, c_f):
        copy.wait_recv()

    after = (
        res_ref[...].astype(F32)
        + (part[x].astype(F32) + from_l[...].astype(F32) + from_r[...].astype(F32))
    ).astype(BF16)
    mixed[...] = after
    tok[core] = norm_rows(after, gain_ref[...][None, :]).astype(BF16)
    t_x = start(remote(tok.at[core], tok.at[core], pair_s.at[1], pair_r.at[1], to_partner))
    m_x.wait_recv()
    keys = meta[...].reshape(2 * rows, meta.shape[2])
    slots = 8 * chips
    wanted = (lax.broadcasted_iota(jnp.int32, (2 * rows, slots), 1) + core * slots).astype(F32)
    first = keys[:, 0:1] == wanted
    second = keys[:, 1:2] == wanted
    choose = (first | second).astype(F32).astype(BF16)
    t_x.wait_recv()

    def select(t, carry):
        source = tok[:, :, cols_of(t)].reshape(2 * rows, COLS)
        picked = lax.dot_general(
            choose, source, (((0,), (0,)), ((), ())), preferred_element_type=F32
        )
        sendb[:, :, cols_of(t)] = picked.reshape(chips, 8, COLS).astype(BF16)
        return carry

    lax.fori_loop(0, tiles, select, 0)
    z_out = [None]
    for p in range(1, chips):
        z_out.append(
            start(
                remote(sendb.at[p], rec.at[x, p], zs.at[p], zr.at[p], on_ring(offsets[p]))
            )
        )
    rec[x, 0] = sendb[0]
    for load in loads:
        load.wait()

    fwd = [None] * n_chunks

    def spread(q):
        for p in range(q * SPAN, (q + 1) * SPAN):
            if p:
                z_out[p].wait_recv()
        whole = pl.ds(q * SPAN, SPAN)
        fwd[q] = [
            start(remote(rec.at[x, whole], rec.at[x, whole], xs.at[q, 0], xr_.at[q, 0], to_right)),
            start(remote(rec.at[x, whole], rec.at[x, whole], xs.at[q, 1], xr_.at[q, 1], to_left)),
        ]

    relays = [None] * n_chunks

    def relay(q):
        a = pl.ds(q * SPAN, SPAN // 2)
        b = pl.ds(q * SPAN + SPAN // 2, SPAN // 2)
        fwd[q][0].wait_recv()
        one = start(remote(rec.at[left, a], rec.at[left, a], xs.at[q, 2], xr_.at[q, 2], to_right))
        fwd[q][1].wait_recv()
        two = start(remote(rec.at[right, b], rec.at[right, b], xs.at[q, 3], xr_.at[q, 3], to_left))
        relays[q] = [one, two]

    backs = [None] * n_chunks
    lo2, hi2 = pl.ds(0, SPAN // 2), pl.ds(SPAN // 2, SPAN // 2)

    def experts(q):
        for copy in relays[q]:
            copy.wait_recv()
        many = 4 * SPAN * 8
        arrived = rec[:, q * SPAN : (q + 1) * SPAN].reshape(many, width)
        gate = dot_nt(arrived, wg_ref[...])
        up = dot_nt(arrived, wu_ref[...])
        hidden = (gate / (1.0 + jnp.exp(-gate)) * up).astype(BF16)

        def down(t, carry):
            value = dot(hidden, wd_ref[:, cols_of(t)])
            back_t[q, :, :, :, cols_of(t)] = value.reshape(4, SPAN, 8, COLS).astype(BF16)
            return carry

        lax.fori_loop(0, tiles, down, 0)
        own = back_t.at[q]
        backs[q] = [
            start(remote(own.at[across, lo2], back_rl.at[q], bs.at[q, 0], br.at[q, 0], to_right)),
            start(remote(own.at[across, hi2], back_rr.at[q], bs.at[q, 1], br.at[q, 1], to_left)),
            start(remote(own.at[right, hi2], back_fl.at[q, hi2], bs.at[q, 2], br.at[q, 2], to_right)),
            start(remote(own.at[left, lo2], back_fr.at[q, lo2], bs.at[q, 3], br.at[q, 3], to_left)),
        ]

    def add_relayed(q):
        backs[q][0].wait_recv()
        back_sr[q] = (
            back_t[q, right, : SPAN // 2].astype(F32) + back_rl[q].astype(F32)
        ).astype(BF16)
        backs[q].append(
            start(remote(back_sr.at[q], back_fl.at[q, lo2], bs.at[q, 4], br.at[q, 4], to_right))
        )
        backs[q][1].wait_recv()
        back_sl[q] = (
            back_t[q, left, SPAN // 2 :].astype(F32) + back_rr[q].astype(F32)
        ).astype(BF16)
        backs[q].append(
            start(remote(back_sl.at[q], back_fr.at[q, hi2], bs.at[q, 5], br.at[q, 5], to_left))
        )

    g_out = [None] * chips

    def give_back(q):
        for copy in backs[q][2:]:
            copy.wait_recv()
        zb[q] = (
            back_t[q, x].astype(F32) + back_fl[q].astype(F32) + back_fr[q].astype(F32)
        ).astype(BF16)
        for k in range(SPAN):
            p = q * SPAN + k
            if p:
                g_out[p] = start(
                    remote(zb.at[q, k], gb.at[p], gs.at[p], gr.at[p], on_ring(-offsets[p]))
                )
            else:
                gb[0] = zb[0, 0]

    stages = (spread, relay, experts, add_relayed, give_back)
    for tick in range(n_chunks + len(stages) - 1):
        for s in reversed(range(len(stages))):
            if 0 <= tick - s < n_chunks:
                stages[s](tick - s)

    for p in range(1, chips):
        g_out[p].wait_recv()
    weigh = jnp.where(first, keys[:, 2:3], 0.0) + jnp.where(second, keys[:, 3:4], 0.0)
    weigh_hi = weigh.astype(BF16)
    weigh_lo = (weigh - weigh_hi.astype(F32)).astype(BF16)

    def combine(t, carry):
        returned = gb[:, :, cols_of(t)].reshape(slots, COLS)
        yb[:, :, cols_of(t)] = (dot(weigh_hi, returned) + dot(weigh_lo, returned)).reshape(
            2, rows, COLS
        )
        return carry

    lax.fori_loop(0, tiles, combine, 0)
    y_x = start(remote(yb.at[1 - core], yrecv, pair_s.at[2], pair_r.at[2], to_partner))
    y_x.wait_recv()
    out_ref[...] = (mixed[...].astype(F32) + (yb[core] + yrecv[...])).astype(out_ref.dtype)
    for copy in sends:
        copy.wait_send()


def mixer(
    attended, w_out, residual, gain, routes, group_weight, logits, w_gate, w_up, w_down, chips
):
    rows, width = residual.shape
    n_chunks = chips // SPAN
    vmem = pl.BlockSpec(memory_space=pltpu.VMEM)
    hbm = pl.BlockSpec(memory_space=pl.ANY)
    half = width // 2
    dma = pltpu.SemaphoreType.DMA
    chunk = (n_chunks, SPAN, 8, width)
    half_chunk = (n_chunks, SPAN // 2, 8, width)
    return pl.pallas_call(
        functools.partial(mixer_kernel, chips),
        out_shape=jax.ShapeDtypeStruct((rows, width), BF16),
        in_specs=[vmem] * 7 + [hbm] * 3,
        out_specs=vmem,
        scratch_shapes=[
            pltpu.VMEM(w_gate.shape, BF16),
            pltpu.VMEM(w_up.shape, BF16),
            pltpu.VMEM(w_down.shape, BF16),
            pltpu.VMEM((4, rows, width), BF16),
            pltpu.VMEM((rows, half), BF16),
            pltpu.VMEM((rows, half), BF16),
            pltpu.VMEM((rows, half), BF16),
            pltpu.VMEM((rows, half), BF16),
            pltpu.VMEM((rows, width), BF16),
            pltpu.VMEM((rows, width), BF16),
            pltpu.VMEM((rows, width), BF16),
            pltpu.VMEM((2, rows, 128), F32),
            pltpu.VMEM((2, rows, width), BF16),
            pltpu.VMEM((chips, 8, width), BF16),
            pltpu.VMEM((4, chips, 8, width), BF16),
            pltpu.VMEM((n_chunks, 4, SPAN, 8, width), BF16),
            pltpu.VMEM(half_chunk, BF16),
            pltpu.VMEM(half_chunk, BF16),
            pltpu.VMEM(half_chunk, BF16),
            pltpu.VMEM(half_chunk, BF16),
            pltpu.VMEM(chunk, BF16),
            pltpu.VMEM(chunk, BF16),
            pltpu.VMEM(chunk, BF16),
            pltpu.VMEM((chips, 8, width), BF16),
            pltpu.VMEM((2, rows, width), F32),
            pltpu.VMEM((rows, width), F32),
            dma((3,)),
            dma((3,)),
            dma((3,)),
            dma((6,)),
            dma((6,)),
            dma((chips,)),
            dma((chips,)),
            dma((n_chunks, 4)),
            dma((n_chunks, 4)),
            dma((n_chunks, 6)),
            dma((n_chunks, 6)),
            dma((chips,)),
            dma((chips,)),
        ],
        compiler_params=pltpu.CompilerParams(
            collective_id=0, has_side_effects=True, vmem_limit_bytes=56 * 1024 * 1024
        ),
    )(attended, w_out, residual, gain, routes, group_weight, logits, w_gate, w_up, w_down)


def on_device(
    residual,
    query_latent,
    kv_latent,
    rotary_key,
    doc_ids,
    query_gain,
    kv_gain,
    w_query_nope,
    w_query_rot,
    w_key_nope,
    w_value,
    w_out,
    ffn_gain,
    w_gate,
    w_up,
    w_down,
    routes,
    group_weight,
    member_logits,
):
    chips = lax.axis_size("sp") // 2
    attended = attention(
        query_latent, kv_latent, rotary_key, doc_ids, query_gain, kv_gain, w_query_nope,
        w_query_rot, w_key_nope, w_value,
    )
    return mixer(
        attended, w_out, residual, ffn_gain, routes.T, group_weight, member_logits.T,
        w_gate[0].T, w_up[0].T, w_down[0], chips,
    )


def solution(mesh):
    return jax.shard_map(
        on_device,
        mesh=mesh,
        in_specs=(
            P(("grp", "sp", "tp"), None),
            P(("grp", "sp"), None),
            P(("grp", "sp"), None),
            P(("grp", "sp"), None),
            P(("grp", "sp")),
            P(),
            P(),
            P(None, "tp"),
            P(None, "tp"),
            P(None, "tp"),
            P(None, "tp"),
            P("tp", None),
            P(),
            P("sp", None, "tp"),
            P("sp", None, "tp"),
            P("sp", "tp", None),
            P(("grp", "sp", "tp"), None),
            P(("grp", "sp", "tp")),
            P(("grp", "sp", "tp"), None),
        ),
        out_specs=P(("grp", "sp", "tp"), None),
        check_vma=False,
    )
```

```python
import functools
import math

import jax
import jax.numpy as jnp
from jax import lax
from jax.experimental import pallas as pl
from jax.experimental.pallas import tpu as pltpu
from jax.sharding import PartitionSpec as P

NOPE = 128
ROPE = 64
VDIM = 128
DOC_MOST = 4352

EPSILON = 1e-06
FLOOR_SCORE = -1e30
MESH = pl.DeviceIdType.MESH
F32 = jnp.float32
BF16 = jnp.bfloat16


def norm_rows(source, gain_vec):
    widened = source.astype(F32)
    return (
        widened
        * lax.rsqrt(jnp.mean(widened * widened, axis=-1, keepdims=True) + EPSILON)
        * gain_vec
    )


def dot(a, b):
    return jnp.dot(a, b, preferred_element_type=F32)


def dot_nt(a, b):
    return lax.dot_general(a, b, (((1,), (1,)), ((), ())), preferred_element_type=F32)


def attention_kernel(
    factor, hops, seed,
    ql_ref, kl_ref, rk_ref, doc_ref, qg_ref, kg_ref, wqn_ref, wqr_ref, wk_ref, wv_ref,
    out_ref,
    kv, keys_ref, values_ref, q_ref, m_ref, l_ref, acc_ref, zs, zr, xs, xr_, ds, dr,
):
    sp = lax.axis_index("sp")
    n_sp = lax.axis_size("sp")
    x = lax.axis_index("tp")
    core = lax.rem(sp, 2)
    z = lax.div(sp, 2)
    right, left, across = lax.rem(x + 1, 4), lax.rem(x + 3, 4), lax.rem(x + 2, 4)
    to_right, to_left, to_partner = {"tp": right}, {"tp": left}, {"sp": sp + 1 - 2 * core}

    def chip_at(offset):
        return {"sp": sp + 2 * offset}

    chips = lax.div(n_sp, 2)

    rows = ql_ref.shape[0]
    heads = q_ref.shape[0]
    latent_width = wk_ref.shape[0]
    quarter = rows // 4

    barrier = pltpu.get_barrier_semaphore()

    def greet(target):
        pl.semaphore_signal(barrier, inc=1, device_id=target, device_id_type=MESH)

    for target in (to_partner, to_left, to_right):
        greet(target)
    for offset in (1, seed):

        @pl.when(z >= offset)
        def _():
            greet(chip_at(-offset))

    has_next = z + 1 < chips
    has_far = z + seed < chips

    def remote(src, dst, ssem, rsem, target):
        return pltpu.make_async_remote_copy(
            src_ref=src, dst_ref=dst, send_sem=ssem, recv_sem=rsem, device_id=target,
            device_id_type=MESH,
        )

    def onward(h):
        return remote(
            kv.at[h, core, x], kv.at[h + 1, core, x], zs.at[h + 1], zr.at[h + 1], chip_at(1)
        )

    def jump():
        return remote(
            kv.at[0, core, x], kv.at[seed, core, x], zs.at[seed], zr.at[seed], chip_at(seed)
        )

    def beside(h, k):
        owner = (x, x, left, right)[k]
        target = (to_right, to_left, to_right, to_left)[k]
        part = kv.at[h, core, owner]
        if k >= 2:
            part = part.at[pl.ds((k - 2) * (quarter // 2), quarter // 2)]
        return remote(part, part, xs.at[h, k], xr_.at[h, k], target)

    def shared(h):
        return [
            remote(
                r.at[h, core], r.at[h, core], ds.at[h, k], dr.at[h, k], to_partner
            )
            for k, r in enumerate((keys_ref, values_ref))
        ]

    step = -math.log(10000.0) / (ROPE // 2)
    frequency = jnp.exp(
        lax.broadcasted_iota(jnp.int32, (ROPE // 2, rows), 0).astype(F32) * step
    )
    position = (sp * rows + lax.broadcasted_iota(jnp.int32, (ROPE // 2, rows), 1)).astype(F32)
    angles = position * frequency
    cosine, sine = jnp.cos(angles), jnp.sin(angles)

    def turned(source):
        a, b = source[: ROPE // 2], source[ROPE // 2 :]
        return jnp.concatenate([a * cosine - b * sine, a * sine + b * cosine], axis=0)

    docs = jnp.broadcast_to(doc_ref[...], (ROPE, rows))
    same_doc = docs == lax.broadcasted_iota(jnp.int32, (ROPE, rows), 0)
    key_tail = jnp.concatenate(
        [turned(rk_ref[...].astype(F32)), same_doc.astype(F32)], axis=0
    ).T.astype(BF16)
    latent = norm_rows(kl_ref[...], kg_ref[...][None, :]).astype(BF16)
    own = jnp.concatenate([latent, key_tail], axis=1)
    kv[0, core] = own.reshape(4, quarter, own.shape[1])
    pl.semaphore_wait(barrier, 3 + has_next.astype(jnp.int32) + has_far.astype(jnp.int32))

    @pl.when(has_next)
    def _():
        onward(0).start()

    @pl.when(has_far)
    def _():
        jump().start()


    def project(h):
        block = kv[h, core].reshape(rows, kv.shape[-1])
        latent = block[:, :latent_width]
        keys_ref[h, core, :, :latent_width] = dot(latent, wk_ref[...]).astype(BF16)
        keys_ref[h, core, :, latent_width:] = block[:, latent_width:]
        values_ref[h, core] = lax.dot_general(
            wv_ref[...], latent, (((0,), (1,)), ((), ())), preferred_element_type=F32
        ).astype(BF16)
        for copy in shared(h):
            copy.start()

    project(0)

    query_normed = norm_rows(ql_ref[...], qg_ref[...][None, :]).astype(BF16)
    nope = lax.dot_general(
        wqn_ref[...], query_normed, (((0,), (1,)), ((), ())), preferred_element_type=F32
    )
    rot = dot_nt(wqr_ref[...], query_normed)
    reject = jnp.where(same_doc, 0.0, FLOOR_SCORE)
    for h in range(heads):
        q_ref[h] = jnp.concatenate(
            [nope[h * NOPE : (h + 1) * NOPE], turned(rot[h * ROPE : (h + 1) * ROPE]), reject],
            axis=0,
        ).astype(BF16)

    def attend(h, blocks, diagonal):
        scores, values = [], []
        for b in blocks:
            keys = keys_ref[h, b]
            tail = keys[:, latent_width:]
            values.append(values_ref[h, b])
            scores.append([
                dot(
                    jnp.concatenate([keys[:, i * NOPE : (i + 1) * NOPE], tail], axis=1), q_ref[i]
                )
                for i in range(heads)
            ])
        if diagonal:
            shape = (rows, rows)
            col = core * rows + lax.broadcasted_iota(jnp.int32, shape, 1)
            row = lax.broadcasted_iota(jnp.int32, shape, 0)
            scores = [
                [jnp.where(row + k * rows <= col, s, FLOOR_SCORE) for s in block]
                for k, block in enumerate(scores)
            ]
        for i in range(heads):
            mine = [block[i] for block in scores]
            highest = functools.reduce(
                jnp.maximum, [jnp.max(s, axis=0, keepdims=True) for s in mine]
            )
            if not diagonal:
                old = m_ref[i]
                highest = jnp.maximum(old, highest)
            weights = [jnp.exp((s - highest) * factor) for s in mine]
            total = sum(jnp.sum(w, axis=0, keepdims=True) for w in weights)
            attended = sum(
                dot(v[i * VDIM : (i + 1) * VDIM], w.astype(BF16)) for v, w in zip(values, weights)
            )
            if not diagonal:
                shrink = jnp.exp((old - highest) * factor)
                total = l_ref[i] * shrink + total
                attended = acc_ref[i] * shrink + attended
            m_ref[i] = highest
            l_ref[i] = total
            acc_ref[i] = attended

    near, far = list(range(1, seed)), list(range(seed, hops + 1))
    order = near[:3] + far[:1] + near[3:] + far[1:]

    def hop_at(n):
        hop = n
        for k, at in enumerate(order):
            hop = jnp.where(n == k + 1, at, hop)
        return hop

    def exists(h):
        return (h >= 1) & (h <= z) & ((h < hops) | ((h == hops) & (core == 1)))

    def goes_on(h):
        more = (h < hops - 1) | ((h == hops - 1) & (core == 1))
        return (h != seed - 1) & more & has_next

    def held(n):
        return (n >= 1) & (n <= hops) & exists(hop_at(n))

    def arrive(n):
        @pl.when(held(n))
        def _():
            h = hop_at(n)
            onward(h - 1).wait_recv()

            @pl.when(goes_on(h))
            def _():
                onward(h).start()

            beside(h, 0).start()
            beside(h, 1).start()

    def pass_on(n):
        @pl.when(held(n))
        def _():
            h = hop_at(n)
            beside(h, 0).wait_recv()
            beside(h, 2).start()
            beside(h, 1).wait_recv()
            beside(h, 3).start()

    def share(n):
        @pl.when(held(n))
        def _():
            h = hop_at(n)
            beside(h, 2).wait_recv()
            beside(h, 3).wait_recv()
            project(h)

    def use(n):
        h = hop_at(n)

        @pl.when((n >= 1) & (n < hops) & (h <= z))
        def _():
            for copy in shared(h):
                copy.wait_recv()
            attend(h, (0, 1), False)

    arrive(1)
    for copy in shared(0):
        copy.wait_recv()
    attend(0, (0, 1), True)

    def tick(t, carry):
        arrive(t)
        pass_on(t - 1)
        share(t - 2)
        use(t - 3)
        return carry

    lax.fori_loop(2, hops + 3, tick, 0)

    @pl.when((core == 0) & (hops <= z))
    def _():
        for copy in shared(hops):
            copy.wait_recv()
        attend(hops, (1,), False)

    for i in range(heads):
        out_ref[:, i * VDIM : (i + 1) * VDIM] = (acc_ref[i] / l_ref[i]).T.astype(out_ref.dtype)

    @pl.when(has_next)
    def _():
        onward(0).wait_send()

    @pl.when(has_far)
    def _():
        jump().wait_send()

    for copy in shared(0):
        copy.wait_send()

    def drain(h, carry):
        @pl.when(exists(h))
        def _():
            @pl.when(goes_on(h))
            def _():
                onward(h).wait_send()

            for k in range(4):
                beside(h, k).wait_send()
            for copy in shared(h):
                copy.wait_send()

        return carry

    lax.fori_loop(1, hops + 1, drain, 0)


def attention(
    query_latent, kv_latent, rotary_key, doc_ids, query_gain, kv_gain, w_query_nope, w_query_rot,
    w_key, w_value,
):
    rows = query_latent.shape[0]
    heads = w_key.shape[1] // NOPE
    width = heads * VDIM
    latent_width = kv_latent.shape[1]
    blocks_back = (DOC_MOST + rows - 2) // rows
    hops = (blocks_back + 1) // 2
    assert blocks_back % 2 == 1 and hops % 2 == 1
    seed = (hops + 1) // 2
    vmem = pl.BlockSpec(memory_space=pltpu.VMEM)
    dma = pltpu.SemaphoreType.DMA
    return pl.pallas_call(
        functools.partial(attention_kernel, (NOPE + ROPE) ** (-0.5), hops, seed),
        out_shape=jax.ShapeDtypeStruct((rows, width), BF16),
        in_specs=[vmem] * 10,
        out_specs=vmem,
        scratch_shapes=[
            pltpu.VMEM((hops + 1, 2, 4, rows // 4, latent_width + 2 * ROPE), BF16),
            pltpu.VMEM((hops + 1, 2, rows, width + 2 * ROPE), BF16),
            pltpu.VMEM((hops + 1, 2, width, rows), BF16),
            pltpu.VMEM((heads, 2 * NOPE, rows), BF16),
            pltpu.VMEM((heads, 1, rows), F32),
            pltpu.VMEM((heads, 1, rows), F32),
            pltpu.VMEM((heads, VDIM, rows), F32),
            dma((hops + 1,)),
            dma((hops + 1,)),
            dma((hops + 1, 4)),
            dma((hops + 1, 4)),
            dma((hops + 1, 2)),
            dma((hops + 1, 2)),
        ],
        compiler_params=pltpu.CompilerParams(
            collective_id=1, has_side_effects=True, vmem_limit_bytes=56 * 1024 * 1024
        ),
    )(
        query_latent, kv_latent, rotary_key.T, doc_ids[None, :],
        query_gain, kv_gain, w_query_nope, w_query_rot.T, w_key, w_value,
    )


COLS = 512
SPAN = 2


def offsets_of(chips):
    half, quarter = chips // 2, chips // 4
    offsets = [0, 1]
    for m in range(1, quarter - 1):
        offsets += [-m, m + 1]
    for m in range(half, quarter - 1, -1):
        offsets += [m, 1 - m]
    return offsets


def mixer_kernel(
    chips,
    att_ref, res_ref, gain_ref, routes_ref, group_ref, logits_ref, wout_hbm, wg_hbm, wu_hbm, wd_hbm,
    out_ref,
    wout_ref, wg_ref, wu_ref, wd_ref, part, relay_l, relay_r, sum_r, sum_l, from_l, from_r, mixed,
    meta, tok, sendb, rec, back_t, back_rl, back_rr, back_sr, back_sl, back_fl, back_fr, zb, gb,
    gb2,
    wsem, pair_s, pair_r, hs, hr, ps, pr, zs, zr, xs, xr_, bs, br, gs, gr,
):
    sp = lax.axis_index("sp")
    x = lax.axis_index("tp")
    core = lax.rem(sp, 2)
    z = lax.div(sp, 2)
    partner = sp + 1 - 2 * core
    right, left, across = lax.rem(x + 1, 4), lax.rem(x + 3, 4), lax.rem(x + 2, 4)
    to_right, to_left, to_partner = {"tp": right}, {"tp": left}, {"sp": partner}
    offsets = offsets_of(chips)
    n_chunks = chips // SPAN
    rows, width = res_ref.shape
    half = width // 2

    def on_ring(offset):
        return {"sp": lax.rem(z + offset + chips, chips) * 2 + core}

    barrier = pltpu.get_barrier_semaphore()
    for target in [to_partner, to_left, to_right] + [on_ring(o) for o in offsets[1:]]:
        pl.semaphore_signal(barrier, inc=1, device_id=target, device_id_type=MESH)

    w_load = pltpu.make_async_copy(wout_hbm, wout_ref, wsem.at[3])
    w_load.start()
    loads = [
        pltpu.make_async_copy(wg_hbm, wg_ref, wsem.at[0]),
        pltpu.make_async_copy(wu_hbm, wu_ref, wsem.at[1]),
        pltpu.make_async_copy(wd_hbm, wd_ref, wsem.at[2]),
    ]
    for load in loads:
        load.start()

    def remote(src, dst, ssem, rsem, target):
        return pltpu.make_async_remote_copy(
            src_ref=src, dst_ref=dst, send_sem=ssem, recv_sem=rsem, device_id=target,
            device_id_type=MESH,
        )

    def cols_of(t):
        return pl.ds(pl.multiple_of(t * COLS, COLS), COLS)

    def project(t, carry):
        value = dot(att_ref[...], wout_ref[:, cols_of(t)])
        part[:, :, cols_of(t)] = value.reshape(4, rows, COLS).astype(BF16)
        return carry

    sends = []

    def start(copy):
        copy.start()
        sends.append(copy)
        return copy

    lo, hi = pl.ds(0, half), pl.ds(half, half)
    tiles = width // COLS
    w_load.wait()
    lax.fori_loop(0, tiles // 2, project, 0)
    pl.semaphore_wait(barrier, 3 + len(offsets) - 1)
    c_a = start(remote(part.at[across, :, lo], relay_l, ps.at[0], pr.at[0], to_right))
    c_d = start(remote(part.at[left, :, lo], from_r.at[:, lo], ps.at[1], pr.at[1], to_left))
    lax.fori_loop(tiles // 2, tiles, project, 0)
    c_b = start(remote(part.at[across, :, hi], relay_r, ps.at[2], pr.at[2], to_left))
    c_c = start(remote(part.at[right, :, hi], from_l.at[:, hi], ps.at[3], pr.at[3], to_right))
    routes = routes_ref[...]
    expert = lax.broadcasted_iota(jnp.int32, (2 * chips, rows), 0)
    goes = [routes[k : k + 1] == expert for k in range(2)]
    earlier = (
        lax.broadcasted_iota(jnp.int32, (rows, rows), 0)
        < lax.broadcasted_iota(jnp.int32, (rows, rows), 1)
    )
    before = dot(
        (goes[0] | goes[1]).astype(F32).astype(BF16), earlier.astype(F32).astype(BF16)
    )
    distance = lax.rem(lax.div(routes, 2) - z + chips, chips)
    place = jnp.zeros_like(routes)
    for p, offset in enumerate(offsets):
        place = jnp.where(distance == offset % chips, p, place)
    spot = (lax.rem(routes, 2) * (8 * chips) + place * 8 + core * 4).astype(F32)
    ranks = [jnp.sum(jnp.where(g, before, 0.0), axis=0, keepdims=True) for g in goes]
    logits = logits_ref[...]
    top = jnp.maximum(logits[0:1], logits[1:2])
    powers = [jnp.exp(logits[k : k + 1] - top) for k in range(2)]
    share = group_ref[...][None, :] / (powers[0] + powers[1])
    table = [spot[k : k + 1] + ranks[k] for k in range(2)] + [p * share for p in powers]
    table.append(jnp.zeros((meta.shape[2] - 4, rows), F32))
    meta[core] = jnp.concatenate(table, axis=0).T

    m_x = start(remote(meta.at[core], meta.at[core], pair_s.at[0], pair_r.at[0], to_partner))
    c_a.wait_recv()
    sum_r[...] = (part[right, :, :half].astype(F32) + relay_l[...].astype(F32)).astype(BF16)
    c_e = start(remote(sum_r, from_l.at[:, lo], ps.at[4], pr.at[4], to_right))
    c_b.wait_recv()
    sum_l[...] = (part[left, :, half:].astype(F32) + relay_r[...].astype(F32)).astype(BF16)
    c_f = start(remote(sum_l, from_r.at[:, hi], ps.at[5], pr.at[5], to_left))
    for copy in (c_d, c_c, c_e, c_f):
        copy.wait_recv()

    after = (
        res_ref[...].astype(F32)
        + (part[x].astype(F32) + from_l[...].astype(F32) + from_r[...].astype(F32))
    ).astype(BF16)
    mixed[...] = after
    tok[core] = norm_rows(after, gain_ref[...][None, :]).astype(BF16)
    t_x = start(remote(tok.at[core], tok.at[core], pair_s.at[1], pair_r.at[1], to_partner))
    m_x.wait_recv()
    keys = meta[...].reshape(2 * rows, meta.shape[2])
    slots = 8 * chips
    wanted = (lax.broadcasted_iota(jnp.int32, (2 * rows, slots), 1) + core * slots).astype(F32)
    first = keys[:, 0:1] == wanted
    second = keys[:, 1:2] == wanted
    choose = (first | second).astype(F32).astype(BF16)
    t_x.wait_recv()

    def select(t, carry):
        source = tok[:, :, cols_of(t)].reshape(2 * rows, COLS)
        picked = lax.dot_general(
            choose, source, (((0,), (0,)), ((), ())), preferred_element_type=F32
        )
        sendb[:, :, cols_of(t)] = picked.reshape(chips, 8, COLS).astype(BF16)
        return carry

    lax.fori_loop(0, tiles, select, 0)
    z_out = [None]
    for p in range(1, chips):
        z_out.append(
            start(
                remote(sendb.at[p], rec.at[x, p], zs.at[p], zr.at[p], on_ring(offsets[p]))
            )
        )
    rec[x, 0] = sendb[0]
    for load in loads:
        load.wait()

    fwd = [None] * n_chunks

    def spread(q):
        for p in range(q * SPAN, (q + 1) * SPAN):
            if p:
                z_out[p].wait_recv()
        whole = pl.ds(q * SPAN, SPAN)
        fwd[q] = [
            start(remote(rec.at[x, whole], rec.at[x, whole], xs.at[q, 0], xr_.at[q, 0], to_right)),
            start(remote(rec.at[x, whole], rec.at[x, whole], xs.at[q, 1], xr_.at[q, 1], to_left)),
        ]

    relays = [None] * n_chunks

    def relay(q):
        a = pl.ds(q * SPAN, SPAN // 2)
        b = pl.ds(q * SPAN + SPAN // 2, SPAN // 2)
        fwd[q][0].wait_recv()
        one = start(remote(rec.at[left, a], rec.at[left, a], xs.at[q, 2], xr_.at[q, 2], to_right))
        fwd[q][1].wait_recv()
        two = start(remote(rec.at[right, b], rec.at[right, b], xs.at[q, 3], xr_.at[q, 3], to_left))
        relays[q] = [one, two]

    backs = [None] * n_chunks
    lo2, hi2 = pl.ds(0, SPAN // 2), pl.ds(SPAN // 2, SPAN // 2)

    def experts(q):
        for copy in relays[q]:
            copy.wait_recv()
        many = 4 * SPAN * 8
        arrived = rec[:, q * SPAN : (q + 1) * SPAN].reshape(many, width)
        gate = dot_nt(arrived, wg_ref[...])
        up = dot_nt(arrived, wu_ref[...])
        hidden = (gate / (1.0 + jnp.exp(-gate)) * up).astype(BF16)

        def down(t, carry):
            value = dot(hidden, wd_ref[:, cols_of(t)])
            back_t[q, :, :, :, cols_of(t)] = value.reshape(4, SPAN, 8, COLS).astype(BF16)
            return carry

        lax.fori_loop(0, tiles, down, 0)
        own = back_t.at[q]
        backs[q] = [
            start(remote(own.at[across, lo2], back_rl.at[q], bs.at[q, 0], br.at[q, 0], to_right)),
            start(remote(own.at[across, hi2], back_rr.at[q], bs.at[q, 1], br.at[q, 1], to_left)),
            start(remote(own.at[right, hi2], back_fl.at[q, hi2], bs.at[q, 2], br.at[q, 2], to_right)),
            start(remote(own.at[left, lo2], back_fr.at[q, lo2], bs.at[q, 3], br.at[q, 3], to_left)),
        ]

    def add_relayed(q):
        backs[q][0].wait_recv()
        back_sr[q] = (
            back_t[q, right, : SPAN // 2].astype(F32) + back_rl[q].astype(F32)
        ).astype(BF16)
        backs[q].append(
            start(remote(back_sr.at[q], back_fl.at[q, lo2], bs.at[q, 4], br.at[q, 4], to_right))
        )
        backs[q][1].wait_recv()
        back_sl[q] = (
            back_t[q, left, SPAN // 2 :].astype(F32) + back_rr[q].astype(F32)
        ).astype(BF16)
        backs[q].append(
            start(remote(back_sl.at[q], back_fr.at[q, hi2], bs.at[q, 5], br.at[q, 5], to_left))
        )

    g_out = [None] * chips

    def give_back(q):
        for copy in backs[q][2:]:
            copy.wait_recv()
        zb[q] = (
            back_t[q, x].astype(F32) + back_fl[q].astype(F32) + back_fr[q].astype(F32)
        ).astype(BF16)
        for k in range(SPAN):
            p = q * SPAN + k
            if p:
                g_out[p] = start(
                    remote(zb.at[q, k], gb.at[p], gs.at[p], gr.at[p], on_ring(-offsets[p]))
                )
            else:
                gb[0] = zb[0, 0]

    stages = (spread, relay, experts, add_relayed, give_back)
    for tick in range(n_chunks + len(stages) - 1):
        for s in reversed(range(len(stages))):
            if 0 <= tick - s < n_chunks:
                stages[s](tick - s)

    across_cores = []
    for p in range(chips):
        if p:
            g_out[p].wait_recv()
        across_cores.append(start(remote(gb.at[p], gb2.at[p], hs.at[p], hr.at[p], to_partner)))
    mine = meta[core]

    def weigh(parity):
        here = (
            lax.broadcasted_iota(jnp.int32, (rows, slots), 1) + parity * slots
        ).astype(F32)
        weight = jnp.where(mine[:, 0:1] == here, mine[:, 2:3], 0.0)
        weight = weight + jnp.where(mine[:, 1:2] == here, mine[:, 3:4], 0.0)
        high = weight.astype(BF16)
        return high, (weight - high.astype(F32)).astype(BF16)

    weights = [weigh(core), weigh(1 - core)]
    for copy in across_cores:
        copy.wait_recv()

    def combine(t, carry):
        routed = 0.0
        for (high, low), blocks in zip(weights, (gb, gb2)):
            returned = blocks[:, :, cols_of(t)].reshape(slots, COLS)
            routed = routed + (dot(high, returned) + dot(low, returned))
        out_ref[:, cols_of(t)] = (mixed[:, cols_of(t)].astype(F32) + routed).astype(out_ref.dtype)
        return carry

    lax.fori_loop(0, tiles, combine, 0)
    for copy in sends:
        copy.wait_send()


def mixer(
    attended, w_out, residual, gain, routes, group_weight, logits, w_gate, w_up, w_down, chips
):
    rows, width = residual.shape
    n_chunks = chips // SPAN
    vmem = pl.BlockSpec(memory_space=pltpu.VMEM)
    hbm = pl.BlockSpec(memory_space=pl.ANY)
    half = width // 2
    dma = pltpu.SemaphoreType.DMA
    chunk = (n_chunks, SPAN, 8, width)
    half_chunk = (n_chunks, SPAN // 2, 8, width)
    return pl.pallas_call(
        functools.partial(mixer_kernel, chips),
        out_shape=jax.ShapeDtypeStruct((rows, width), BF16),
        in_specs=[vmem] * 6 + [hbm] * 4,
        out_specs=vmem,
        scratch_shapes=[
            pltpu.VMEM(w_out.shape, BF16),
            pltpu.VMEM(w_gate.shape, BF16),
            pltpu.VMEM(w_up.shape, BF16),
            pltpu.VMEM(w_down.shape, BF16),
            pltpu.VMEM((4, rows, width), BF16),
            pltpu.VMEM((rows, half), BF16),
            pltpu.VMEM((rows, half), BF16),
            pltpu.VMEM((rows, half), BF16),
            pltpu.VMEM((rows, half), BF16),
            pltpu.VMEM((rows, width), BF16),
            pltpu.VMEM((rows, width), BF16),
            pltpu.VMEM((rows, width), BF16),
            pltpu.VMEM((2, rows, 128), F32),
            pltpu.VMEM((2, rows, width), BF16),
            pltpu.VMEM((chips, 8, width), BF16),
            pltpu.VMEM((4, chips, 8, width), BF16),
            pltpu.VMEM((n_chunks, 4, SPAN, 8, width), BF16),
            pltpu.VMEM(half_chunk, BF16),
            pltpu.VMEM(half_chunk, BF16),
            pltpu.VMEM(half_chunk, BF16),
            pltpu.VMEM(half_chunk, BF16),
            pltpu.VMEM(chunk, BF16),
            pltpu.VMEM(chunk, BF16),
            pltpu.VMEM(chunk, BF16),
            pltpu.VMEM((chips, 8, width), BF16),
            pltpu.VMEM((chips, 8, width), BF16),
            dma((4,)),
            dma((2,)),
            dma((2,)),
            dma((chips,)),
            dma((chips,)),
            dma((6,)),
            dma((6,)),
            dma((chips,)),
            dma((chips,)),
            dma((n_chunks, 4)),
            dma((n_chunks, 4)),
            dma((n_chunks, 6)),
            dma((n_chunks, 6)),
            dma((chips,)),
            dma((chips,)),
        ],
        compiler_params=pltpu.CompilerParams(
            collective_id=0, has_side_effects=True, vmem_limit_bytes=56 * 1024 * 1024
        ),
    )(attended, residual, gain, routes, group_weight, logits, w_out, w_gate, w_up, w_down)


def on_device(
    residual,
    query_latent,
    kv_latent,
    rotary_key,
    doc_ids,
    query_gain,
    kv_gain,
    w_query_nope,
    w_query_rot,
    w_key_nope,
    w_value,
    w_out,
    ffn_gain,
    w_gate,
    w_up,
    w_down,
    routes,
    group_weight,
    member_logits,
):
    chips = lax.axis_size("sp") // 2
    attended = attention(
        query_latent, kv_latent, rotary_key, doc_ids, query_gain, kv_gain, w_query_nope,
        w_query_rot, w_key_nope, w_value,
    )
    return mixer(
        attended, w_out, residual, ffn_gain, routes.T, group_weight, member_logits.T,
        w_gate[0].T, w_up[0].T, w_down[0], chips,
    )


def solution(mesh):
    return jax.shard_map(
        on_device,
        mesh=mesh,
        in_specs=(
            P(("grp", "sp", "tp"), None),
            P(("grp", "sp"), None),
            P(("grp", "sp"), None),
            P(("grp", "sp"), None),
            P(("grp", "sp")),
            P(),
            P(),
            P(None, "tp"),
            P(None, "tp"),
            P(None, "tp"),
            P(None, "tp"),
            P("tp", None),
            P(),
            P("sp", None, "tp"),
            P("sp", None, "tp"),
            P("sp", "tp", None),
            P(("grp", "sp", "tp"), None),
            P(("grp", "sp", "tp")),
            P(("grp", "sp", "tp"), None),
        ),
        out_specs=P(("grp", "sp", "tp"), None),
        check_vma=False,
    )
```

```python
import functools
import math

import jax
import jax.numpy as jnp
from jax import lax
from jax.experimental import pallas as pl
from jax.experimental.pallas import tpu as pltpu
from jax.sharding import PartitionSpec as P

NOPE = 128
ROPE = 64
VDIM = 128
DOC_MOST = 4352

EPSILON = 1e-06
FLOOR_SCORE = -1e30
MESH = pl.DeviceIdType.MESH
F32 = jnp.float32
BF16 = jnp.bfloat16


def norm_rows(source, gain_vec):
    widened = source.astype(F32)
    return (
        widened
        * lax.rsqrt(jnp.mean(widened * widened, axis=-1, keepdims=True) + EPSILON)
        * gain_vec
    )


def dot(a, b):
    return jnp.dot(a, b, preferred_element_type=F32)


def dot_nt(a, b):
    return lax.dot_general(a, b, (((1,), (1,)), ((), ())), preferred_element_type=F32)


def attention_kernel(
    factor, hops,
    ql_ref, kl_ref, rk_ref, doc_ref, qg_ref, kg_ref, wqn_ref, wqr_ref, wk_ref, wv_ref,
    out_ref,
    kv, keys_ref, values_ref, q_ref, m_ref, l_ref, acc_ref, zs, zr, xs, xr_, ds, dr,
):
    sp = lax.axis_index("sp")
    n_sp = lax.axis_size("sp")
    x = lax.axis_index("tp")
    core = lax.rem(sp, 2)
    z = lax.div(sp, 2)
    right, left, across = lax.rem(x + 1, 4), lax.rem(x + 3, 4), lax.rem(x + 2, 4)
    to_right, to_left, to_partner = {"tp": right}, {"tp": left}, {"sp": sp + 1 - 2 * core}

    def chip_at(offset):
        return {"sp": sp + 2 * offset}

    chips = lax.div(n_sp, 2)

    rows = ql_ref.shape[0]
    heads = q_ref.shape[0]
    latent_width = wk_ref.shape[0]
    quarter = rows // 4

    barrier = pltpu.get_barrier_semaphore()

    def greet(target):
        pl.semaphore_signal(barrier, inc=1, device_id=target, device_id_type=MESH)

    for target in (to_partner, to_left, to_right):
        greet(target)

    @pl.when(z >= 1)
    def _():
        greet(chip_at(-1))

    has_next = z + 1 < chips

    def remote(src, dst, ssem, rsem, target):
        return pltpu.make_async_remote_copy(
            src_ref=src, dst_ref=dst, send_sem=ssem, recv_sem=rsem, device_id=target,
            device_id_type=MESH,
        )

    def onward(h, k):
        piece = pl.ds(k * (quarter // 2), quarter // 2)
        return remote(
            kv.at[h, core, x, piece], kv.at[h + 1, core, x, piece], zs.at[h + 1, k],
            zr.at[h + 1, k], chip_at(1),
        )

    def beside(h, k):
        owner = (x, x, left, right)[k]
        target = (to_right, to_left, to_right, to_left)[k]
        part = kv.at[h, core, owner]
        if k >= 2:
            part = part.at[pl.ds((k - 2) * (quarter // 2), quarter // 2)]
        return remote(part, part, xs.at[h, k], xr_.at[h, k], target)

    def shared(h):
        return [
            remote(
                r.at[h, core], r.at[h, core], ds.at[h, k], dr.at[h, k], to_partner
            )
            for k, r in enumerate((keys_ref, values_ref))
        ]

    step = -math.log(10000.0) / (ROPE // 2)
    frequency = jnp.exp(
        lax.broadcasted_iota(jnp.int32, (ROPE // 2, rows), 0).astype(F32) * step
    )
    position = (sp * rows + lax.broadcasted_iota(jnp.int32, (ROPE // 2, rows), 1)).astype(F32)
    angles = position * frequency
    cosine, sine = jnp.cos(angles), jnp.sin(angles)

    def turned(source):
        a, b = source[: ROPE // 2], source[ROPE // 2 :]
        return jnp.concatenate([a * cosine - b * sine, a * sine + b * cosine], axis=0)

    docs = jnp.broadcast_to(doc_ref[...], (ROPE, rows))
    same_doc = docs == lax.broadcasted_iota(jnp.int32, (ROPE, rows), 0)
    key_tail = jnp.concatenate(
        [turned(rk_ref[...].astype(F32)), same_doc.astype(F32)], axis=0
    ).T.astype(BF16)
    latent = norm_rows(kl_ref[...], kg_ref[...][None, :]).astype(BF16)
    own = jnp.concatenate([latent, key_tail], axis=1)
    kv[0, core] = own.reshape(4, quarter, own.shape[1])
    pl.semaphore_wait(barrier, 3 + has_next.astype(jnp.int32))

    @pl.when(has_next)
    def _():
        onward(0, 0).start()
        onward(0, 1).start()


    def project(h):
        block = kv[h, core].reshape(rows, kv.shape[-1])
        latent = block[:, :latent_width]
        keys_ref[h, core, :, :latent_width] = dot(latent, wk_ref[...]).astype(BF16)
        keys_ref[h, core, :, latent_width:] = block[:, latent_width:]
        values_ref[h, core] = lax.dot_general(
            wv_ref[...], latent, (((0,), (1,)), ((), ())), preferred_element_type=F32
        ).astype(BF16)
        for copy in shared(h):
            copy.start()

    project(0)

    query_normed = norm_rows(ql_ref[...], qg_ref[...][None, :]).astype(BF16)
    nope = lax.dot_general(
        wqn_ref[...], query_normed, (((0,), (1,)), ((), ())), preferred_element_type=F32
    )
    rot = dot_nt(wqr_ref[...], query_normed)
    reject = jnp.where(same_doc, 0.0, FLOOR_SCORE)
    for h in range(heads):
        q_ref[h] = jnp.concatenate(
            [nope[h * NOPE : (h + 1) * NOPE], turned(rot[h * ROPE : (h + 1) * ROPE]), reject],
            axis=0,
        ).astype(BF16)

    def attend(h, blocks, diagonal):
        scores, values = [], []
        for b in blocks:
            keys = keys_ref[h, b]
            tail = keys[:, latent_width:]
            values.append(values_ref[h, b])
            scores.append([
                dot(
                    jnp.concatenate([keys[:, i * NOPE : (i + 1) * NOPE], tail], axis=1), q_ref[i]
                )
                for i in range(heads)
            ])
        if diagonal:
            shape = (rows, rows)
            col = core * rows + lax.broadcasted_iota(jnp.int32, shape, 1)
            row = lax.broadcasted_iota(jnp.int32, shape, 0)
            scores = [
                [jnp.where(row + k * rows <= col, s, FLOOR_SCORE) for s in block]
                for k, block in enumerate(scores)
            ]
        for i in range(heads):
            mine = [block[i] for block in scores]
            highest = functools.reduce(
                jnp.maximum, [jnp.max(s, axis=0, keepdims=True) for s in mine]
            )
            if not diagonal:
                old = m_ref[i]
                highest = jnp.maximum(old, highest)
            weights = [jnp.exp((s - highest) * factor) for s in mine]
            total = sum(jnp.sum(w, axis=0, keepdims=True) for w in weights)
            attended = sum(
                dot(v[i * VDIM : (i + 1) * VDIM], w.astype(BF16)) for v, w in zip(values, weights)
            )
            if not diagonal:
                shrink = jnp.exp((old - highest) * factor)
                total = l_ref[i] * shrink + total
                attended = acc_ref[i] * shrink + attended
            m_ref[i] = highest
            l_ref[i] = total
            acc_ref[i] = attended

    def exists(h):
        return (h >= 1) & (h <= z) & ((h < hops) | ((h == hops) & (core == 1)))

    def goes_on(h):
        more = (h < hops - 1) | ((h == hops - 1) & (core == 1))
        return more & has_next

    def arrive(h):
        @pl.when(exists(h))
        def _():
            for k in range(2):
                onward(h - 1, k).wait_recv()

                @pl.when(goes_on(h))
                def _():
                    onward(h, k).start()

            beside(h, 0).start()
            beside(h, 1).start()

    def pass_on(h):
        @pl.when(exists(h))
        def _():
            beside(h, 0).wait_recv()
            beside(h, 2).start()
            beside(h, 1).wait_recv()
            beside(h, 3).start()

    def share(h):
        @pl.when(exists(h))
        def _():
            beside(h, 2).wait_recv()
            beside(h, 3).wait_recv()
            project(h)

    def use(h):
        @pl.when((h >= 1) & (h < hops) & (h <= z))
        def _():
            for copy in shared(h):
                copy.wait_recv()
            attend(h, (0, 1), False)

    arrive(1)
    for copy in shared(0):
        copy.wait_recv()
    attend(0, (0, 1), True)

    def tick(t, carry):
        arrive(t)
        pass_on(t - 1)
        share(t - 3)
        use(t - 4)
        return carry

    lax.fori_loop(2, hops + 4, tick, 0)

    @pl.when((core == 0) & (hops <= z))
    def _():
        for copy in shared(hops):
            copy.wait_recv()
        attend(hops, (1,), False)

    for i in range(heads):
        out_ref[:, i * VDIM : (i + 1) * VDIM] = (acc_ref[i] / l_ref[i]).T.astype(out_ref.dtype)

    @pl.when(has_next)
    def _():
        onward(0, 0).wait_send()
        onward(0, 1).wait_send()

    for copy in shared(0):
        copy.wait_send()

    def drain(h, carry):
        @pl.when(exists(h))
        def _():
            @pl.when(goes_on(h))
            def _():
                onward(h, 0).wait_send()
                onward(h, 1).wait_send()

            for k in range(4):
                beside(h, k).wait_send()
            for copy in shared(h):
                copy.wait_send()

        return carry

    lax.fori_loop(1, hops + 1, drain, 0)


def attention(
    query_latent, kv_latent, rotary_key, doc_ids, query_gain, kv_gain, w_query_nope, w_query_rot,
    w_key, w_value,
):
    rows = query_latent.shape[0]
    heads = w_key.shape[1] // NOPE
    width = heads * VDIM
    latent_width = kv_latent.shape[1]
    blocks_back = (DOC_MOST + rows - 2) // rows
    hops = (blocks_back + 1) // 2
    assert blocks_back % 2 == 1
    vmem = pl.BlockSpec(memory_space=pltpu.VMEM)
    dma = pltpu.SemaphoreType.DMA
    return pl.pallas_call(
        functools.partial(attention_kernel, (NOPE + ROPE) ** (-0.5), hops),
        out_shape=jax.ShapeDtypeStruct((rows, width), BF16),
        in_specs=[vmem] * 10,
        out_specs=vmem,
        scratch_shapes=[
            pltpu.VMEM((hops + 1, 2, 4, rows // 4, latent_width + 2 * ROPE), BF16),
            pltpu.VMEM((hops + 1, 2, rows, width + 2 * ROPE), BF16),
            pltpu.VMEM((hops + 1, 2, width, rows), BF16),
            pltpu.VMEM((heads, 2 * NOPE, rows), BF16),
            pltpu.VMEM((heads, 1, rows), F32),
            pltpu.VMEM((heads, 1, rows), F32),
            pltpu.VMEM((heads, VDIM, rows), F32),
            dma((hops + 1, 2)),
            dma((hops + 1, 2)),
            dma((hops + 1, 4)),
            dma((hops + 1, 4)),
            dma((hops + 1, 2)),
            dma((hops + 1, 2)),
        ],
        compiler_params=pltpu.CompilerParams(
            collective_id=1, has_side_effects=True, vmem_limit_bytes=56 * 1024 * 1024
        ),
    )(
        query_latent, kv_latent, rotary_key.T, doc_ids[None, :],
        query_gain, kv_gain, w_query_nope, w_query_rot.T, w_key, w_value,
    )


COLS = 512
SPAN = 2


def offsets_of(chips):
    half, quarter = chips // 2, chips // 4
    offsets = [0, 1]
    for m in range(1, quarter - 1):
        offsets += [-m, m + 1]
    for m in range(half - 1, quarter + 1, -1):
        offsets += [m, -m]
    return offsets[: half + 2] + [half, -quarter - 1, quarter + 1, -quarter, quarter, 1 - quarter]


def mixer_kernel(
    chips,
    att_ref, res_ref, gain_ref, routes_ref, group_ref, logits_ref, wout_hbm, wg_hbm, wu_hbm, wd_hbm,
    out_ref,
    wout_ref, wg_ref, wu_ref, wd_ref, part, relay_l, relay_r, sum_r, sum_l, from_l, from_r, mixed,
    meta, tok, sendb, rec, back_t, back_rl, back_rr, back_sr, back_sl, back_fl, back_fr, zb, gb,
    gb2, way, way_back,
    wsem, wosem, ws, wr, pair_s, pair_r, hs, hr, ps, pr, zs, zr, xs, xr_, bs, br, gs, gr,
):
    sp = lax.axis_index("sp")
    x = lax.axis_index("tp")
    core = lax.rem(sp, 2)
    z = lax.div(sp, 2)
    partner = sp + 1 - 2 * core
    right, left, across = lax.rem(x + 1, 4), lax.rem(x + 3, 4), lax.rem(x + 2, 4)
    to_right, to_left, to_partner = {"tp": right}, {"tp": left}, {"sp": partner}
    offsets = offsets_of(chips)
    n_chunks = chips // SPAN
    rows, width = res_ref.shape
    half = width // 2

    def on_ring(offset):
        return {"sp": lax.rem(z + offset + chips, chips) * 2 + core}

    barrier = pltpu.get_barrier_semaphore()
    for target in [to_partner, to_left, to_right] + [on_ring(o) for o in offsets[1:]]:
        pl.semaphore_signal(barrier, inc=1, device_id=target, device_id_type=MESH)

    tiles = width // COLS

    def cols_of(t):
        return pl.ds(pl.multiple_of(t * COLS, COLS), COLS)

    def w_load(t):
        return pltpu.make_async_copy(
            wout_hbm.at[:, cols_of(t)], wout_ref.at[:, cols_of(t)], wosem.at[t]
        )

    for t in range(tiles):
        w_load(t).start()
    loads = [
        pltpu.make_async_copy(wg_hbm, wg_ref, wsem.at[0]),
        pltpu.make_async_copy(wu_hbm, wu_ref, wsem.at[1]),
        pltpu.make_async_copy(wd_hbm, wd_ref, wsem.at[2]),
    ]

    def remote(src, dst, ssem, rsem, target):
        return pltpu.make_async_remote_copy(
            src_ref=src, dst_ref=dst, send_sem=ssem, recv_sem=rsem, device_id=target,
            device_id_type=MESH,
        )

    def project(t, carry):
        w_load(t).wait()
        value = dot(att_ref[...], wout_ref[:, cols_of(t)])
        part[:, :, cols_of(t)] = value.reshape(4, rows, COLS).astype(BF16)
        return carry

    sends = []

    def start(copy):
        copy.start()
        sends.append(copy)
        return copy

    lo, hi = pl.ds(0, half), pl.ds(half, half)
    lax.fori_loop(0, tiles // 2, project, 0)
    pl.semaphore_wait(barrier, 3 + len(offsets) - 1)
    c_a = start(remote(part.at[across, :, lo], relay_l, ps.at[0], pr.at[0], to_right))
    c_d = start(remote(part.at[left, :, lo], from_r.at[:, lo], ps.at[1], pr.at[1], to_left))
    lax.fori_loop(tiles // 2, tiles, project, 0)
    for load in loads:
        load.start()
    c_b = start(remote(part.at[across, :, hi], relay_r, ps.at[2], pr.at[2], to_left))
    c_c = start(remote(part.at[right, :, hi], from_l.at[:, hi], ps.at[3], pr.at[3], to_right))
    routes = routes_ref[...]
    expert = lax.broadcasted_iota(jnp.int32, (2 * chips, rows), 0)
    goes = [routes[k : k + 1] == expert for k in range(2)]
    earlier = (
        lax.broadcasted_iota(jnp.int32, (rows, rows), 0)
        < lax.broadcasted_iota(jnp.int32, (rows, rows), 1)
    )
    before = dot(
        (goes[0] | goes[1]).astype(F32).astype(BF16), earlier.astype(F32).astype(BF16)
    )
    distance = lax.rem(lax.div(routes, 2) - z + chips, chips)
    place = jnp.zeros_like(routes)
    for p, offset in enumerate(offsets):
        place = jnp.where(distance == offset % chips, p, place)
    spot = (lax.rem(routes, 2) * (8 * chips) + place * 8 + core * 4).astype(F32)
    ranks = [jnp.sum(jnp.where(g, before, 0.0), axis=0, keepdims=True) for g in goes]
    logits = logits_ref[...]
    top = jnp.maximum(logits[0:1], logits[1:2])
    powers = [jnp.exp(logits[k : k + 1] - top) for k in range(2)]
    share = group_ref[...][None, :] / (powers[0] + powers[1])
    table = [spot[k : k + 1] + ranks[k] for k in range(2)] + [p * share for p in powers]
    table.append(jnp.zeros((meta.shape[2] - 4, rows), F32))
    meta[core] = jnp.concatenate(table, axis=0).T

    m_x = start(remote(meta.at[core], meta.at[core], pair_s.at[0], pair_r.at[0], to_partner))
    c_a.wait_recv()
    sum_r[...] = (part[right, :, :half].astype(F32) + relay_l[...].astype(F32)).astype(BF16)
    c_e = start(remote(sum_r, from_l.at[:, lo], ps.at[4], pr.at[4], to_right))
    c_b.wait_recv()
    sum_l[...] = (part[left, :, half:].astype(F32) + relay_r[...].astype(F32)).astype(BF16)
    c_f = start(remote(sum_l, from_r.at[:, hi], ps.at[5], pr.at[5], to_left))
    for copy in (c_d, c_c, c_e, c_f):
        copy.wait_recv()

    after = (
        res_ref[...].astype(F32)
        + (part[x].astype(F32) + from_l[...].astype(F32) + from_r[...].astype(F32))
    ).astype(BF16)
    mixed[...] = after
    tok[core] = norm_rows(after, gain_ref[...][None, :]).astype(BF16)
    t_x = start(remote(tok.at[core], tok.at[core], pair_s.at[1], pair_r.at[1], to_partner))
    m_x.wait_recv()
    keys = meta[...].reshape(2 * rows, meta.shape[2])
    slots = 8 * chips
    wanted = (lax.broadcasted_iota(jnp.int32, (2 * rows, slots), 1) + core * slots).astype(F32)
    first = keys[:, 0:1] == wanted
    second = keys[:, 1:2] == wanted
    choose = (first | second).astype(F32).astype(BF16)
    t_x.wait_recv()

    def select(t, carry):
        source = tok[:, :, cols_of(t)].reshape(2 * rows, COLS)
        picked = lax.dot_general(
            choose, source, (((0,), (0,)), ((), ())), preferred_element_type=F32
        )
        sendb[:, :, cols_of(t)] = picked.reshape(chips, 8, COLS).astype(BF16)
        return carry

    opposite = offsets.index(chips // 2)
    quarter = chips // 4

    def both_ways(block, buffers, first, ssems, rsems):
        return [
            start(
                remote(
                    block.at[:, cols], buffers.at[k], ssems.at[first + k], rsems.at[first + k],
                    on_ring(side * quarter),
                )
            )
            for k, (cols, side) in enumerate(((lo, 1), (hi, -1)))
        ]

    def hand_on(arriving, buffers, block):
        base = 0 if buffers is way else 4
        for k, (cols, side) in enumerate(((lo, 1), (hi, -1))):
            arriving[k].wait_recv()
            arriving.append(
                start(
                    remote(
                        buffers.at[k], block.at[:, cols], ws.at[base + 2 + k],
                        wr.at[base + 2 + k], on_ring(side * quarter),
                    )
                )
            )

    def arrived_in_full(copies):
        for copy in copies[2:] if isinstance(copies, list) else [copies]:
            copy.wait_recv()

    lax.fori_loop(0, tiles, select, 0)
    z_out = [None]
    z_out += [None] * (chips - 1)
    near = list(range(1, 6))
    for p in near + [opposite] + [p for p in range(6, chips) if p != opposite]:
        if p == opposite:
            z_out[p] = both_ways(sendb.at[p], way, 0, ws, wr)
        else:
            z_out[p] = start(
                remote(sendb.at[p], rec.at[x, p], zs.at[p], zr.at[p], on_ring(offsets[p]))
            )
    rec[x, 0] = sendb[0]
    for load in loads:
        load.wait()

    fwd = [None] * n_chunks

    def spread(q):
        for p in range(q * SPAN, (q + 1) * SPAN):
            if p:
                arrived_in_full(z_out[p])
        whole = pl.ds(q * SPAN, SPAN)
        fwd[q] = [
            start(remote(rec.at[x, whole], rec.at[x, whole], xs.at[q, 0], xr_.at[q, 0], to_right)),
            start(remote(rec.at[x, whole], rec.at[x, whole], xs.at[q, 1], xr_.at[q, 1], to_left)),
        ]

    relays = [None] * n_chunks

    def relay(q):
        a = pl.ds(q * SPAN, SPAN // 2)
        b = pl.ds(q * SPAN + SPAN // 2, SPAN // 2)
        fwd[q][0].wait_recv()
        one = start(remote(rec.at[left, a], rec.at[left, a], xs.at[q, 2], xr_.at[q, 2], to_right))
        fwd[q][1].wait_recv()
        two = start(remote(rec.at[right, b], rec.at[right, b], xs.at[q, 3], xr_.at[q, 3], to_left))
        relays[q] = [one, two]

    backs = [None] * n_chunks
    lo2, hi2 = pl.ds(0, SPAN // 2), pl.ds(SPAN // 2, SPAN // 2)

    def experts(q):
        for copy in relays[q]:
            copy.wait_recv()
        many = 4 * SPAN * 8
        arrived = rec[:, q * SPAN : (q + 1) * SPAN].reshape(many, width)
        gate = dot_nt(arrived, wg_ref[...])
        up = dot_nt(arrived, wu_ref[...])
        hidden = (gate / (1.0 + jnp.exp(-gate)) * up).astype(BF16)

        def down(t, carry):
            value = dot(hidden, wd_ref[:, cols_of(t)])
            back_t[q, :, :, :, cols_of(t)] = value.reshape(4, SPAN, 8, COLS).astype(BF16)
            return carry

        lax.fori_loop(0, tiles, down, 0)
        own = back_t.at[q]
        backs[q] = [
            start(remote(own.at[across, lo2], back_rl.at[q], bs.at[q, 0], br.at[q, 0], to_right)),
            start(remote(own.at[across, hi2], back_rr.at[q], bs.at[q, 1], br.at[q, 1], to_left)),
            start(remote(own.at[right, hi2], back_fl.at[q, hi2], bs.at[q, 2], br.at[q, 2], to_right)),
            start(remote(own.at[left, lo2], back_fr.at[q, lo2], bs.at[q, 3], br.at[q, 3], to_left)),
        ]

    def add_relayed(q):
        backs[q][0].wait_recv()
        back_sr[q] = (
            back_t[q, right, : SPAN // 2].astype(F32) + back_rl[q].astype(F32)
        ).astype(BF16)
        backs[q].append(
            start(remote(back_sr.at[q], back_fl.at[q, lo2], bs.at[q, 4], br.at[q, 4], to_right))
        )
        backs[q][1].wait_recv()
        back_sl[q] = (
            back_t[q, left, SPAN // 2 :].astype(F32) + back_rr[q].astype(F32)
        ).astype(BF16)
        backs[q].append(
            start(remote(back_sl.at[q], back_fr.at[q, hi2], bs.at[q, 5], br.at[q, 5], to_left))
        )

    g_out = [None] * chips

    def give_back(q):
        for copy in backs[q][2:]:
            copy.wait_recv()
        zb[q] = (
            back_t[q, x].astype(F32) + back_fl[q].astype(F32) + back_fr[q].astype(F32)
        ).astype(BF16)
        for k in range(SPAN):
            p = q * SPAN + k
            if p == opposite:
                g_out[p] = both_ways(zb.at[q, k], way_back, 4, ws, wr)
            elif p:
                g_out[p] = start(
                    remote(zb.at[q, k], gb.at[p], gs.at[p], gr.at[p], on_ring(-offsets[p]))
                )
            else:
                gb[0] = zb[0, 0]

    stages = ((give_back, 4), (add_relayed, 3), (experts, 2), (relay, 1), (spread, 0))
    opposite_chunk = opposite // SPAN
    for tick in range(n_chunks + 4):
        if tick == 2:
            hand_on(z_out[opposite], way, rec.at[x, opposite])
        if tick == opposite_chunk + 5:
            hand_on(g_out[opposite], way_back, gb.at[opposite])
        for stage, lag in stages:
            if 0 <= tick - lag < n_chunks:
                stage(tick - lag)

    across_cores = []
    for p in range(chips):
        if p:
            arrived_in_full(g_out[p])
        across_cores.append(start(remote(gb.at[p], gb2.at[p], hs.at[p], hr.at[p], to_partner)))
    mine = meta[core]

    def weigh(parity):
        here = (
            lax.broadcasted_iota(jnp.int32, (rows, slots), 1) + parity * slots
        ).astype(F32)
        weight = jnp.where(mine[:, 0:1] == here, mine[:, 2:3], 0.0)
        weight = weight + jnp.where(mine[:, 1:2] == here, mine[:, 3:4], 0.0)
        high = weight.astype(BF16)
        return high, (weight - high.astype(F32)).astype(BF16)

    weights = [weigh(core), weigh(1 - core)]
    for copy in across_cores:
        copy.wait_recv()

    def combine(t, carry):
        routed = 0.0
        for (high, low), blocks in zip(weights, (gb, gb2)):
            returned = blocks[:, :, cols_of(t)].reshape(slots, COLS)
            routed = routed + (dot(high, returned) + dot(low, returned))
        out_ref[:, cols_of(t)] = (mixed[:, cols_of(t)].astype(F32) + routed).astype(out_ref.dtype)
        return carry

    lax.fori_loop(0, tiles, combine, 0)
    for copy in sends:
        copy.wait_send()


def mixer(
    attended, w_out, residual, gain, routes, group_weight, logits, w_gate, w_up, w_down, chips
):
    rows, width = residual.shape
    n_chunks = chips // SPAN
    vmem = pl.BlockSpec(memory_space=pltpu.VMEM)
    hbm = pl.BlockSpec(memory_space=pl.ANY)
    half = width // 2
    dma = pltpu.SemaphoreType.DMA
    chunk = (n_chunks, SPAN, 8, width)
    half_chunk = (n_chunks, SPAN // 2, 8, width)
    return pl.pallas_call(
        functools.partial(mixer_kernel, chips),
        out_shape=jax.ShapeDtypeStruct((rows, width), BF16),
        in_specs=[vmem] * 6 + [hbm] * 4,
        out_specs=vmem,
        scratch_shapes=[
            pltpu.VMEM(w_out.shape, BF16),
            pltpu.VMEM(w_gate.shape, BF16),
            pltpu.VMEM(w_up.shape, BF16),
            pltpu.VMEM(w_down.shape, BF16),
            pltpu.VMEM((4, rows, width), BF16),
            pltpu.VMEM((rows, half), BF16),
            pltpu.VMEM((rows, half), BF16),
            pltpu.VMEM((rows, half), BF16),
            pltpu.VMEM((rows, half), BF16),
            pltpu.VMEM((rows, width), BF16),
            pltpu.VMEM((rows, width), BF16),
            pltpu.VMEM((rows, width), BF16),
            pltpu.VMEM((2, rows, 128), F32),
            pltpu.VMEM((2, rows, width), BF16),
            pltpu.VMEM((chips, 8, width), BF16),
            pltpu.VMEM((4, chips, 8, width), BF16),
            pltpu.VMEM((n_chunks, 4, SPAN, 8, width), BF16),
            pltpu.VMEM(half_chunk, BF16),
            pltpu.VMEM(half_chunk, BF16),
            pltpu.VMEM(half_chunk, BF16),
            pltpu.VMEM(half_chunk, BF16),
            pltpu.VMEM(chunk, BF16),
            pltpu.VMEM(chunk, BF16),
            pltpu.VMEM(chunk, BF16),
            pltpu.VMEM((chips, 8, width), BF16),
            pltpu.VMEM((chips, 8, width), BF16),
            pltpu.VMEM((2, 8, half), BF16),
            pltpu.VMEM((2, 8, half), BF16),
            dma((3,)),
            dma((width // COLS,)),
            dma((8,)),
            dma((8,)),
            dma((2,)),
            dma((2,)),
            dma((chips,)),
            dma((chips,)),
            dma((6,)),
            dma((6,)),
            dma((chips,)),
            dma((chips,)),
            dma((n_chunks, 4)),
            dma((n_chunks, 4)),
            dma((n_chunks, 6)),
            dma((n_chunks, 6)),
            dma((chips,)),
            dma((chips,)),
        ],
        compiler_params=pltpu.CompilerParams(
            collective_id=0, has_side_effects=True, vmem_limit_bytes=56 * 1024 * 1024
        ),
    )(attended, residual, gain, routes, group_weight, logits, w_out, w_gate, w_up, w_down)


def on_device(
    residual,
    query_latent,
    kv_latent,
    rotary_key,
    doc_ids,
    query_gain,
    kv_gain,
    w_query_nope,
    w_query_rot,
    w_key_nope,
    w_value,
    w_out,
    ffn_gain,
    w_gate,
    w_up,
    w_down,
    routes,
    group_weight,
    member_logits,
):
    chips = lax.axis_size("sp") // 2
    attended = attention(
        query_latent, kv_latent, rotary_key, doc_ids, query_gain, kv_gain, w_query_nope,
        w_query_rot, w_key_nope, w_value,
    )
    return mixer(
        attended, w_out, residual, ffn_gain, routes.T, group_weight, member_logits.T,
        w_gate[0].T, w_up[0].T, w_down[0], chips,
    )


def solution(mesh):
    return jax.shard_map(
        on_device,
        mesh=mesh,
        in_specs=(
            P(("grp", "sp", "tp"), None),
            P(("grp", "sp"), None),
            P(("grp", "sp"), None),
            P(("grp", "sp"), None),
            P(("grp", "sp")),
            P(),
            P(),
            P(None, "tp"),
            P(None, "tp"),
            P(None, "tp"),
            P(None, "tp"),
            P("tp", None),
            P(),
            P("sp", None, "tp"),
            P("sp", None, "tp"),
            P("sp", "tp", None),
            P(("grp", "sp", "tp"), None),
            P(("grp", "sp", "tp")),
            P(("grp", "sp", "tp"), None),
        ),
        out_specs=P(("grp", "sp", "tp"), None),
        check_vma=False,
    )
```

```python
import functools
import math

import jax
import jax.numpy as jnp
from jax import lax
from jax.experimental import pallas as pl
from jax.experimental.pallas import tpu as pltpu
from jax.sharding import PartitionSpec as P

NOPE = 128
ROPE = 64
VDIM = 128
DOC_MOST = 4352

EPSILON = 1e-06
FLOOR_SCORE = -1e30
MESH = pl.DeviceIdType.MESH
F32 = jnp.float32
BF16 = jnp.bfloat16


def norm_rows(source, gain_vec):
    widened = source.astype(F32)
    return (
        widened
        * lax.rsqrt(jnp.mean(widened * widened, axis=-1, keepdims=True) + EPSILON)
        * gain_vec
    )


def dot(a, b):
    return jnp.dot(a, b, preferred_element_type=F32)


def dot_nt(a, b):
    return lax.dot_general(a, b, (((1,), (1,)), ((), ())), preferred_element_type=F32)


def attention_kernel(
    factor, hops,
    ql_ref, kl_ref, rk_ref, doc_ref, qg_ref, kg_ref, wqn_ref, wqr_ref, wk_ref, wv_ref,
    out_ref,
    kv, keys_ref, values_ref, q_ref, m_ref, l_ref, acc_ref, zs, zr, xs, xr_, ds, dr,
):
    sp = lax.axis_index("sp")
    n_sp = lax.axis_size("sp")
    x = lax.axis_index("tp")
    core = lax.rem(sp, 2)
    z = lax.div(sp, 2)
    right, left, across = lax.rem(x + 1, 4), lax.rem(x + 3, 4), lax.rem(x + 2, 4)
    to_right, to_left, to_partner = {"tp": right}, {"tp": left}, {"sp": sp + 1 - 2 * core}

    def chip_at(offset):
        return {"sp": sp + 2 * offset}

    chips = lax.div(n_sp, 2)

    rows = ql_ref.shape[0]
    heads = q_ref.shape[0]
    latent_width = wk_ref.shape[0]
    quarter = rows // 4

    barrier = pltpu.get_barrier_semaphore()

    def greet(target):
        pl.semaphore_signal(barrier, inc=1, device_id=target, device_id_type=MESH)

    for target in (to_partner, to_left, to_right):
        greet(target)

    @pl.when(z >= 1)
    def _():
        greet(chip_at(-1))

    has_next = z + 1 < chips

    def remote(src, dst, ssem, rsem, target):
        return pltpu.make_async_remote_copy(
            src_ref=src, dst_ref=dst, send_sem=ssem, recv_sem=rsem, device_id=target,
            device_id_type=MESH,
        )

    def onward(h, k):
        piece = pl.ds(k * (quarter // 2), quarter // 2)
        return remote(
            kv.at[h, core, x, piece], kv.at[h + 1, core, x, piece], zs.at[h + 1, k],
            zr.at[h + 1, k], chip_at(1),
        )

    def beside(h, k):
        owner = (x, x, left, right)[k]
        target = (to_right, to_left, to_right, to_left)[k]
        part = kv.at[h, core, owner]
        if k >= 2:
            part = part.at[pl.ds((k - 2) * (quarter // 2), quarter // 2)]
        return remote(part, part, xs.at[h, k], xr_.at[h, k], target)

    def shared(h):
        return [
            remote(
                r.at[h, core], r.at[h, core], ds.at[h, k], dr.at[h, k], to_partner
            )
            for k, r in enumerate((keys_ref, values_ref))
        ]

    step = -math.log(10000.0) / (ROPE // 2)
    frequency = jnp.exp(
        lax.broadcasted_iota(jnp.int32, (ROPE // 2, rows), 0).astype(F32) * step
    )
    position = (sp * rows + lax.broadcasted_iota(jnp.int32, (ROPE // 2, rows), 1)).astype(F32)
    angles = position * frequency
    cosine, sine = jnp.cos(angles), jnp.sin(angles)

    def turned(source):
        a, b = source[: ROPE // 2], source[ROPE // 2 :]
        return jnp.concatenate([a * cosine - b * sine, a * sine + b * cosine], axis=0)

    docs = jnp.broadcast_to(doc_ref[...], (ROPE, rows))
    same_doc = docs == lax.broadcasted_iota(jnp.int32, (ROPE, rows), 0)
    key_tail = jnp.concatenate(
        [turned(rk_ref[...].astype(F32)), same_doc.astype(F32)], axis=0
    ).T.astype(BF16)
    latent = norm_rows(kl_ref[...], kg_ref[...][None, :]).astype(BF16)
    own = jnp.concatenate([latent, key_tail], axis=1)
    kv[0, core] = own.reshape(4, quarter, own.shape[1])
    pl.semaphore_wait(barrier, 3 + has_next.astype(jnp.int32))

    @pl.when(has_next)
    def _():
        onward(0, 0).start()
        onward(0, 1).start()


    def project(h):
        block = kv[h, core].reshape(rows, kv.shape[-1])
        latent = block[:, :latent_width]
        keys_ref[h, core, :, :latent_width] = dot(latent, wk_ref[...]).astype(BF16)
        keys_ref[h, core, :, latent_width:] = block[:, latent_width:]
        values_ref[h, core] = lax.dot_general(
            wv_ref[...], latent, (((0,), (1,)), ((), ())), preferred_element_type=F32
        ).astype(BF16)
        for copy in shared(h):
            copy.start()

    project(0)

    query_normed = norm_rows(ql_ref[...], qg_ref[...][None, :]).astype(BF16)
    nope = lax.dot_general(
        wqn_ref[...], query_normed, (((0,), (1,)), ((), ())), preferred_element_type=F32
    )
    rot = dot_nt(wqr_ref[...], query_normed)
    reject = jnp.where(same_doc, 0.0, FLOOR_SCORE)
    for h in range(heads):
        q_ref[h] = jnp.concatenate(
            [nope[h * NOPE : (h + 1) * NOPE], turned(rot[h * ROPE : (h + 1) * ROPE]), reject],
            axis=0,
        ).astype(BF16)

    def attend(h, blocks, diagonal):
        scores, values = [], []
        for b in blocks:
            keys = keys_ref[h, b]
            tail = keys[:, latent_width:]
            values.append(values_ref[h, b])
            scores.append([
                dot(
                    jnp.concatenate([keys[:, i * NOPE : (i + 1) * NOPE], tail], axis=1), q_ref[i]
                )
                for i in range(heads)
            ])
        if diagonal:
            shape = (rows, rows)
            col = core * rows + lax.broadcasted_iota(jnp.int32, shape, 1)
            row = lax.broadcasted_iota(jnp.int32, shape, 0)
            scores = [
                [jnp.where(row + k * rows <= col, s, FLOOR_SCORE) for s in block]
                for k, block in enumerate(scores)
            ]
        for i in range(heads):
            mine = [block[i] for block in scores]
            highest = functools.reduce(
                jnp.maximum, [jnp.max(s, axis=0, keepdims=True) for s in mine]
            )
            if not diagonal:
                old = m_ref[i]
                highest = jnp.maximum(old, highest)
            weights = [jnp.exp((s - highest) * factor) for s in mine]
            total = sum(jnp.sum(w, axis=0, keepdims=True) for w in weights)
            attended = sum(
                dot(v[i * VDIM : (i + 1) * VDIM], w.astype(BF16)) for v, w in zip(values, weights)
            )
            if not diagonal:
                shrink = jnp.exp((old - highest) * factor)
                total = l_ref[i] * shrink + total
                attended = acc_ref[i] * shrink + attended
            m_ref[i] = highest
            l_ref[i] = total
            acc_ref[i] = attended

    def exists(h):
        return (h >= 1) & (h <= z) & ((h < hops) | ((h == hops) & (core == 1)))

    def goes_on(h):
        more = (h < hops - 1) | ((h == hops - 1) & (core == 1))
        return more & has_next

    def arrive(h):
        @pl.when(exists(h))
        def _():
            for k in range(2):
                onward(h - 1, k).wait_recv()

                @pl.when(goes_on(h))
                def _():
                    onward(h, k).start()

            beside(h, 0).start()
            beside(h, 1).start()

    def pass_on(h):
        @pl.when(exists(h))
        def _():
            beside(h, 0).wait_recv()
            beside(h, 2).start()
            beside(h, 1).wait_recv()
            beside(h, 3).start()

    def share(h):
        @pl.when(exists(h))
        def _():
            beside(h, 2).wait_recv()
            beside(h, 3).wait_recv()
            project(h)

    def use(h):
        @pl.when((h >= 1) & (h < hops) & (h <= z))
        def _():
            for copy in shared(h):
                copy.wait_recv()
            attend(h, (0, 1), False)

    arrive(1)
    for copy in shared(0):
        copy.wait_recv()
    attend(0, (0, 1), True)

    def tick(t, carry):
        arrive(t)
        pass_on(t - 1)
        share(t - 3)
        use(t - 4)
        return carry

    lax.fori_loop(2, hops + 4, tick, 0)

    @pl.when((core == 0) & (hops <= z))
    def _():
        for copy in shared(hops):
            copy.wait_recv()
        attend(hops, (1,), False)

    for i in range(heads):
        out_ref[:, i * VDIM : (i + 1) * VDIM] = (acc_ref[i] / l_ref[i]).T.astype(out_ref.dtype)

    @pl.when(has_next)
    def _():
        onward(0, 0).wait_send()
        onward(0, 1).wait_send()

    for copy in shared(0):
        copy.wait_send()

    def drain(h, carry):
        @pl.when(exists(h))
        def _():
            @pl.when(goes_on(h))
            def _():
                onward(h, 0).wait_send()
                onward(h, 1).wait_send()

            for k in range(4):
                beside(h, k).wait_send()
            for copy in shared(h):
                copy.wait_send()

        return carry

    lax.fori_loop(1, hops + 1, drain, 0)


def attention(
    query_latent, kv_latent, rotary_key, doc_ids, query_gain, kv_gain, w_query_nope, w_query_rot,
    w_key, w_value,
):
    rows = query_latent.shape[0]
    heads = w_key.shape[1] // NOPE
    width = heads * VDIM
    latent_width = kv_latent.shape[1]
    blocks_back = (DOC_MOST + rows - 2) // rows
    hops = (blocks_back + 1) // 2
    assert blocks_back % 2 == 1
    vmem = pl.BlockSpec(memory_space=pltpu.VMEM)
    dma = pltpu.SemaphoreType.DMA
    return pl.pallas_call(
        functools.partial(attention_kernel, (NOPE + ROPE) ** (-0.5), hops),
        out_shape=jax.ShapeDtypeStruct((rows, width), BF16),
        in_specs=[vmem] * 10,
        out_specs=vmem,
        scratch_shapes=[
            pltpu.VMEM((hops + 1, 2, 4, rows // 4, latent_width + 2 * ROPE), BF16),
            pltpu.VMEM((hops + 1, 2, rows, width + 2 * ROPE), BF16),
            pltpu.VMEM((hops + 1, 2, width, rows), BF16),
            pltpu.VMEM((heads, 2 * NOPE, rows), BF16),
            pltpu.VMEM((heads, 1, rows), F32),
            pltpu.VMEM((heads, 1, rows), F32),
            pltpu.VMEM((heads, VDIM, rows), F32),
            dma((hops + 1, 2)),
            dma((hops + 1, 2)),
            dma((hops + 1, 4)),
            dma((hops + 1, 4)),
            dma((hops + 1, 2)),
            dma((hops + 1, 2)),
        ],
        compiler_params=pltpu.CompilerParams(
            collective_id=1, has_side_effects=True, vmem_limit_bytes=56 * 1024 * 1024
        ),
    )(
        query_latent, kv_latent, rotary_key.T, doc_ids[None, :],
        query_gain, kv_gain, w_query_nope, w_query_rot.T, w_key, w_value,
    )


COLS = 512
SPAN = 2


def offsets_of(chips):
    half, quarter = chips // 2, chips // 4
    offsets = [0, 1, -2, 3]
    for m in range(half - 1, quarter, -1):
        offsets += [m, -m]
    offsets += [half, -quarter]
    for m in range(quarter, 3, -1):
        offsets += [m, 1 - m]
    return offsets + [2, -1]


def mixer_kernel(
    chips,
    att_ref, res_ref, gain_ref, routes_ref, group_ref, logits_ref, wout_hbm, wg_hbm, wu_hbm, wd_hbm,
    out_ref,
    wout_ref, wg_ref, wu_ref, wd_ref, part, relay_l, relay_r, sum_r, sum_l, from_l, from_r, mixed,
    meta, tok, sendb, rec, back_t, back_rl, back_rr, back_sr, back_sl, back_fl, back_fr, zb, gb,
    gb2, way, way_back, outb,
    wsem, wosem, osem, ws, wr, pair_s, pair_r, hs, hr, ps, pr, zs, zr, xs, xr_, bs, br, gs, gr,
):
    sp = lax.axis_index("sp")
    x = lax.axis_index("tp")
    core = lax.rem(sp, 2)
    z = lax.div(sp, 2)
    partner = sp + 1 - 2 * core
    right, left, across = lax.rem(x + 1, 4), lax.rem(x + 3, 4), lax.rem(x + 2, 4)
    to_right, to_left, to_partner = {"tp": right}, {"tp": left}, {"sp": partner}
    offsets = offsets_of(chips)
    n_chunks = chips // SPAN
    rows, width = res_ref.shape
    half = width // 2

    def on_ring(offset):
        return {"sp": lax.rem(z + offset + chips, chips) * 2 + core}

    barrier = pltpu.get_barrier_semaphore()
    for target in [to_partner, to_left, to_right] + [on_ring(o) for o in offsets[1:]]:
        pl.semaphore_signal(barrier, inc=1, device_id=target, device_id_type=MESH)

    tiles = width // COLS

    def cols_of(t):
        return pl.ds(pl.multiple_of(t * COLS, COLS), COLS)

    def w_load(t):
        return pltpu.make_async_copy(
            wout_hbm.at[:, cols_of(t)], wout_ref.at[:, cols_of(t)], wosem.at[t]
        )

    for t in range(tiles):
        w_load(t).start()
    loads = [
        pltpu.make_async_copy(wg_hbm, wg_ref, wsem.at[0]),
        pltpu.make_async_copy(wu_hbm, wu_ref, wsem.at[1]),
        pltpu.make_async_copy(wd_hbm, wd_ref, wsem.at[2]),
    ]

    def remote(src, dst, ssem, rsem, target):
        return pltpu.make_async_remote_copy(
            src_ref=src, dst_ref=dst, send_sem=ssem, recv_sem=rsem, device_id=target,
            device_id_type=MESH,
        )

    def project(t, carry):
        w_load(t).wait()
        value = dot(att_ref[...], wout_ref[:, cols_of(t)])
        part[:, :, cols_of(t)] = value.reshape(4, rows, COLS).astype(BF16)
        return carry

    sends = []

    def start(copy):
        copy.start()
        sends.append(copy)
        return copy

    lo, hi = pl.ds(0, half), pl.ds(half, half)
    lax.fori_loop(0, tiles // 2, project, 0)
    pl.semaphore_wait(barrier, 3 + len(offsets) - 1)
    c_a = start(remote(part.at[across, :, lo], relay_l, ps.at[0], pr.at[0], to_right))
    c_d = start(remote(part.at[left, :, lo], from_r.at[:, lo], ps.at[1], pr.at[1], to_left))
    lax.fori_loop(tiles // 2, tiles, project, 0)
    for load in loads:
        load.start()
    c_b = start(remote(part.at[across, :, hi], relay_r, ps.at[2], pr.at[2], to_left))
    c_c = start(remote(part.at[right, :, hi], from_l.at[:, hi], ps.at[3], pr.at[3], to_right))
    routes = routes_ref[...]
    expert = lax.broadcasted_iota(jnp.int32, (2 * chips, rows), 0)
    goes = [routes[k : k + 1] == expert for k in range(2)]
    earlier = (
        lax.broadcasted_iota(jnp.int32, (rows, rows), 0)
        < lax.broadcasted_iota(jnp.int32, (rows, rows), 1)
    )
    before = dot(
        (goes[0] | goes[1]).astype(F32).astype(BF16), earlier.astype(F32).astype(BF16)
    )
    distance = lax.rem(lax.div(routes, 2) - z + chips, chips)
    place = jnp.zeros_like(routes)
    for p, offset in enumerate(offsets):
        place = jnp.where(distance == offset % chips, p, place)
    spot = (lax.rem(routes, 2) * (8 * chips) + place * 8 + core * 4).astype(F32)
    ranks = [jnp.sum(jnp.where(g, before, 0.0), axis=0, keepdims=True) for g in goes]
    logits = logits_ref[...]
    top = jnp.maximum(logits[0:1], logits[1:2])
    powers = [jnp.exp(logits[k : k + 1] - top) for k in range(2)]
    share = group_ref[...][None, :] / (powers[0] + powers[1])
    table = [spot[k : k + 1] + ranks[k] for k in range(2)] + [p * share for p in powers]
    table.append(jnp.zeros((meta.shape[2] - 4, rows), F32))
    meta[core] = jnp.concatenate(table, axis=0).T

    m_x = start(remote(meta.at[core], meta.at[core], pair_s.at[0], pair_r.at[0], to_partner))
    c_a.wait_recv()
    sum_r[...] = (part[right, :, :half].astype(F32) + relay_l[...].astype(F32)).astype(BF16)
    c_e = start(remote(sum_r, from_l.at[:, lo], ps.at[4], pr.at[4], to_right))
    c_b.wait_recv()
    sum_l[...] = (part[left, :, half:].astype(F32) + relay_r[...].astype(F32)).astype(BF16)
    c_f = start(remote(sum_l, from_r.at[:, hi], ps.at[5], pr.at[5], to_left))
    for copy in (c_d, c_c, c_e, c_f):
        copy.wait_recv()

    after = (
        res_ref[...].astype(F32)
        + (part[x].astype(F32) + from_l[...].astype(F32) + from_r[...].astype(F32))
    ).astype(BF16)
    mixed[...] = after
    tok[core] = norm_rows(after, gain_ref[...][None, :]).astype(BF16)
    t_x = start(remote(tok.at[core], tok.at[core], pair_s.at[1], pair_r.at[1], to_partner))
    m_x.wait_recv()
    keys = meta[...].reshape(2 * rows, meta.shape[2])
    slots = 8 * chips
    wanted = (lax.broadcasted_iota(jnp.int32, (2 * rows, slots), 1) + core * slots).astype(F32)
    first = keys[:, 0:1] == wanted
    second = keys[:, 1:2] == wanted
    choose = (first | second).astype(F32).astype(BF16)
    t_x.wait_recv()

    def select(t, carry):
        source = tok[:, :, cols_of(t)].reshape(2 * rows, COLS)
        picked = lax.dot_general(
            choose, source, (((0,), (0,)), ((), ())), preferred_element_type=F32
        )
        sendb[:, :, cols_of(t)] = picked.reshape(chips, 8, COLS).astype(BF16)
        return carry

    opposite = offsets.index(chips // 2)
    quarter = chips // 4

    def both_ways(block, buffers, first, ssems, rsems):
        return [
            start(
                remote(
                    block.at[:, cols], buffers.at[k], ssems.at[first + k], rsems.at[first + k],
                    on_ring(side * quarter),
                )
            )
            for k, (cols, side) in enumerate(((lo, 1), (hi, -1)))
        ]

    def hand_on(arriving, buffers, block):
        base = 0 if buffers is way else 4
        for k, (cols, side) in enumerate(((lo, 1), (hi, -1))):
            arriving[k].wait_recv()
            arriving.append(
                start(
                    remote(
                        buffers.at[k], block.at[:, cols], ws.at[base + 2 + k],
                        wr.at[base + 2 + k], on_ring(side * quarter),
                    )
                )
            )

    def arrived_in_full(copies):
        for copy in copies[2:] if isinstance(copies, list) else [copies]:
            copy.wait_recv()

    lax.fori_loop(0, tiles, select, 0)
    z_out = [None]
    z_out += [None] * (chips - 1)

    def send_blocks(positions):
        for p in positions:
            z_out[p] = start(
                remote(sendb.at[p], rec.at[x, p], zs.at[p], zr.at[p], on_ring(offsets[p]))
            )

    send_blocks(range(1, SPAN * 2))
    z_out[opposite] = both_ways(sendb.at[opposite], way, 0, ws, wr)
    send_blocks(range(SPAN * 2, opposite))
    rec[x, 0] = sendb[0]
    for load in loads:
        load.wait()

    fwd = [None] * n_chunks

    def spread(q):
        for p in range(q * SPAN, (q + 1) * SPAN):
            if p:
                arrived_in_full(z_out[p])
        whole = pl.ds(q * SPAN, SPAN)
        fwd[q] = [
            start(remote(rec.at[x, whole], rec.at[x, whole], xs.at[q, 0], xr_.at[q, 0], to_right)),
            start(remote(rec.at[x, whole], rec.at[x, whole], xs.at[q, 1], xr_.at[q, 1], to_left)),
        ]

    relays = [None] * n_chunks

    def relay(q):
        a = pl.ds(q * SPAN, SPAN // 2)
        b = pl.ds(q * SPAN + SPAN // 2, SPAN // 2)
        fwd[q][0].wait_recv()
        one = start(remote(rec.at[left, a], rec.at[left, a], xs.at[q, 2], xr_.at[q, 2], to_right))
        fwd[q][1].wait_recv()
        two = start(remote(rec.at[right, b], rec.at[right, b], xs.at[q, 3], xr_.at[q, 3], to_left))
        relays[q] = [one, two]

    backs = [None] * n_chunks
    lo2, hi2 = pl.ds(0, SPAN // 2), pl.ds(SPAN // 2, SPAN // 2)

    def experts(q):
        for copy in relays[q]:
            copy.wait_recv()
        many = 4 * SPAN * 8
        arrived = rec[:, q * SPAN : (q + 1) * SPAN].reshape(many, width)
        gate = dot_nt(arrived, wg_ref[...])
        up = dot_nt(arrived, wu_ref[...])
        hidden = (gate / (1.0 + jnp.exp(-gate)) * up).astype(BF16)

        def down(t, carry):
            value = dot(hidden, wd_ref[:, cols_of(t)])
            back_t[q, :, :, :, cols_of(t)] = value.reshape(4, SPAN, 8, COLS).astype(BF16)
            return carry

        lax.fori_loop(0, tiles, down, 0)
        own = back_t.at[q]
        backs[q] = [
            start(remote(own.at[across, lo2], back_rl.at[q], bs.at[q, 0], br.at[q, 0], to_right)),
            start(remote(own.at[across, hi2], back_rr.at[q], bs.at[q, 1], br.at[q, 1], to_left)),
            start(remote(own.at[right, hi2], back_fl.at[q, hi2], bs.at[q, 2], br.at[q, 2], to_right)),
            start(remote(own.at[left, lo2], back_fr.at[q, lo2], bs.at[q, 3], br.at[q, 3], to_left)),
        ]

    def add_relayed(q):
        backs[q][0].wait_recv()
        back_sr[q] = (
            back_t[q, right, : SPAN // 2].astype(F32) + back_rl[q].astype(F32)
        ).astype(BF16)
        backs[q].append(
            start(remote(back_sr.at[q], back_fl.at[q, lo2], bs.at[q, 4], br.at[q, 4], to_right))
        )
        backs[q][1].wait_recv()
        back_sl[q] = (
            back_t[q, left, SPAN // 2 :].astype(F32) + back_rr[q].astype(F32)
        ).astype(BF16)
        backs[q].append(
            start(remote(back_sl.at[q], back_fr.at[q, hi2], bs.at[q, 5], br.at[q, 5], to_left))
        )

    g_out = [None] * chips

    def give_back(q):
        for copy in backs[q][2:]:
            copy.wait_recv()
        zb[q] = (
            back_t[q, x].astype(F32) + back_fl[q].astype(F32) + back_fr[q].astype(F32)
        ).astype(BF16)
        for k in range(SPAN):
            p = q * SPAN + k
            if p == opposite:
                g_out[p] = both_ways(zb.at[q, k], way_back, 4, ws, wr)
            elif p:
                g_out[p] = start(
                    remote(zb.at[q, k], gb.at[p], gs.at[p], gr.at[p], on_ring(-offsets[p]))
                )
            else:
                gb[0] = zb[0, 0]

    stages = ((give_back, 4), (add_relayed, 3), (experts, 2), (relay, 1), (spread, 0))
    opposite_chunk = opposite // SPAN
    for tick in range(n_chunks + 4):
        if tick == 2:
            hand_on(z_out[opposite], way, rec.at[x, opposite])
            send_blocks(range(opposite + 1, chips))
        if tick == opposite_chunk + 5:
            hand_on(g_out[opposite], way_back, gb.at[opposite])
        for stage, lag in stages:
            if 0 <= tick - lag < n_chunks:
                stage(tick - lag)

    across_cores = []
    for p in range(chips):
        if p:
            arrived_in_full(g_out[p])
        across_cores.append(start(remote(gb.at[p], gb2.at[p], hs.at[p], hr.at[p], to_partner)))
    mine = meta[core]

    def weigh(parity):
        here = (
            lax.broadcasted_iota(jnp.int32, (rows, slots), 1) + parity * slots
        ).astype(F32)
        weight = jnp.where(mine[:, 0:1] == here, mine[:, 2:3], 0.0)
        weight = weight + jnp.where(mine[:, 1:2] == here, mine[:, 3:4], 0.0)
        high = weight.astype(BF16)
        return high, (weight - high.astype(F32)).astype(BF16)

    weights = [weigh(core), weigh(1 - core)]
    for copy in across_cores:
        copy.wait_recv()

    def combine(t, carry):
        routed = 0.0
        for (high, low), blocks in zip(weights, (gb, gb2)):
            returned = blocks[:, :, cols_of(t)].reshape(slots, COLS)
            routed = routed + (dot(high, returned) + dot(low, returned))
        outb[:, cols_of(t)] = (mixed[:, cols_of(t)].astype(F32) + routed).astype(outb.dtype)
        put_out(t).start()
        return carry

    def put_out(t):
        return pltpu.make_async_copy(
            outb.at[:, cols_of(t)], out_ref.at[:, cols_of(t)], osem.at[t]
        )

    lax.fori_loop(0, tiles, combine, 0)
    for t in range(tiles):
        put_out(t).wait()
    for copy in sends:
        copy.wait_send()


def mixer(
    attended, w_out, residual, gain, routes, group_weight, logits, w_gate, w_up, w_down, chips
):
    rows, width = residual.shape
    n_chunks = chips // SPAN
    vmem = pl.BlockSpec(memory_space=pltpu.VMEM)
    hbm = pl.BlockSpec(memory_space=pl.ANY)
    half = width // 2
    dma = pltpu.SemaphoreType.DMA
    chunk = (n_chunks, SPAN, 8, width)
    half_chunk = (n_chunks, SPAN // 2, 8, width)
    return pl.pallas_call(
        functools.partial(mixer_kernel, chips),
        out_shape=jax.ShapeDtypeStruct((rows, width), BF16),
        in_specs=[vmem] * 6 + [hbm] * 4,
        out_specs=hbm,
        scratch_shapes=[
            pltpu.VMEM(w_out.shape, BF16),
            pltpu.VMEM(w_gate.shape, BF16),
            pltpu.VMEM(w_up.shape, BF16),
            pltpu.VMEM(w_down.shape, BF16),
            pltpu.VMEM((4, rows, width), BF16),
            pltpu.VMEM((rows, half), BF16),
            pltpu.VMEM((rows, half), BF16),
            pltpu.VMEM((rows, half), BF16),
            pltpu.VMEM((rows, half), BF16),
            pltpu.VMEM((rows, width), BF16),
            pltpu.VMEM((rows, width), BF16),
            pltpu.VMEM((rows, width), BF16),
            pltpu.VMEM((2, rows, 128), F32),
            pltpu.VMEM((2, rows, width), BF16),
            pltpu.VMEM((chips, 8, width), BF16),
            pltpu.VMEM((4, chips, 8, width), BF16),
            pltpu.VMEM((n_chunks, 4, SPAN, 8, width), BF16),
            pltpu.VMEM(half_chunk, BF16),
            pltpu.VMEM(half_chunk, BF16),
            pltpu.VMEM(half_chunk, BF16),
            pltpu.VMEM(half_chunk, BF16),
            pltpu.VMEM(chunk, BF16),
            pltpu.VMEM(chunk, BF16),
            pltpu.VMEM(chunk, BF16),
            pltpu.VMEM((chips, 8, width), BF16),
            pltpu.VMEM((chips, 8, width), BF16),
            pltpu.VMEM((2, 8, half), BF16),
            pltpu.VMEM((2, 8, half), BF16),
            pltpu.VMEM((rows, width), BF16),
            dma((3,)),
            dma((width // COLS,)),
            dma((width // COLS,)),
            dma((8,)),
            dma((8,)),
            dma((2,)),
            dma((2,)),
            dma((chips,)),
            dma((chips,)),
            dma((6,)),
            dma((6,)),
            dma((chips,)),
            dma((chips,)),
            dma((n_chunks, 4)),
            dma((n_chunks, 4)),
            dma((n_chunks, 6)),
            dma((n_chunks, 6)),
            dma((chips,)),
            dma((chips,)),
        ],
        compiler_params=pltpu.CompilerParams(
            collective_id=0, has_side_effects=True, vmem_limit_bytes=56 * 1024 * 1024
        ),
    )(attended, residual, gain, routes, group_weight, logits, w_out, w_gate, w_up, w_down)


def on_device(
    residual,
    query_latent,
    kv_latent,
    rotary_key,
    doc_ids,
    query_gain,
    kv_gain,
    w_query_nope,
    w_query_rot,
    w_key_nope,
    w_value,
    w_out,
    ffn_gain,
    w_gate,
    w_up,
    w_down,
    routes,
    group_weight,
    member_logits,
):
    chips = lax.axis_size("sp") // 2
    attended = attention(
        query_latent, kv_latent, rotary_key, doc_ids, query_gain, kv_gain, w_query_nope,
        w_query_rot, w_key_nope, w_value,
    )
    return mixer(
        attended, w_out, residual, ffn_gain, routes.T, group_weight, member_logits.T,
        w_gate[0].T, w_up[0].T, w_down[0], chips,
    )


def solution(mesh):
    return jax.shard_map(
        on_device,
        mesh=mesh,
        in_specs=(
            P(("grp", "sp", "tp"), None),
            P(("grp", "sp"), None),
            P(("grp", "sp"), None),
            P(("grp", "sp"), None),
            P(("grp", "sp")),
            P(),
            P(),
            P(None, "tp"),
            P(None, "tp"),
            P(None, "tp"),
            P(None, "tp"),
            P("tp", None),
            P(),
            P("sp", None, "tp"),
            P("sp", None, "tp"),
            P("sp", "tp", None),
            P(("grp", "sp", "tp"), None),
            P(("grp", "sp", "tp")),
            P(("grp", "sp", "tp"), None),
        ),
        out_specs=P(("grp", "sp", "tp"), None),
        check_vma=False,
    )
```

```python
import functools
import math

import jax
import jax.numpy as jnp
from jax import lax
from jax.experimental import pallas as pl
from jax.experimental.pallas import tpu as pltpu
from jax.sharding import PartitionSpec as P

NOPE = 128
ROPE = 64
VDIM = 128
DOC_MOST = 4352

EPSILON = 1e-06
FLOOR_SCORE = -1e30
MESH = pl.DeviceIdType.MESH
F32 = jnp.float32
BF16 = jnp.bfloat16


def norm_rows(source, gain_vec):
    widened = source.astype(F32)
    return (
        widened
        * lax.rsqrt(jnp.mean(widened * widened, axis=-1, keepdims=True) + EPSILON)
        * gain_vec
    )


def dot(a, b):
    return jnp.dot(a, b, preferred_element_type=F32)


def dot_nt(a, b):
    return lax.dot_general(a, b, (((1,), (1,)), ((), ())), preferred_element_type=F32)


def attention_kernel(
    factor, hops,
    ql_ref, kl_ref, rk_ref, doc_ref, qg_ref, kg_ref, wqn_ref, wqr_ref, wk_ref, wv_ref,
    out_ref,
    kv, keys_ref, values_ref, q_ref, m_ref, l_ref, acc_ref, zs, zr, xs, xr_, ds, dr,
):
    sp = lax.axis_index("sp")
    n_sp = lax.axis_size("sp")
    x = lax.axis_index("tp")
    core = lax.rem(sp, 2)
    z = lax.div(sp, 2)
    right, left, across = lax.rem(x + 1, 4), lax.rem(x + 3, 4), lax.rem(x + 2, 4)
    to_right, to_left, to_partner = {"tp": right}, {"tp": left}, {"sp": sp + 1 - 2 * core}

    def chip_at(offset):
        return {"sp": sp + 2 * offset}

    chips = lax.div(n_sp, 2)

    rows = ql_ref.shape[0]
    heads = q_ref.shape[0]
    latent_width = wk_ref.shape[0]
    quarter = rows // 4

    barrier = pltpu.get_barrier_semaphore()

    def greet(target):
        pl.semaphore_signal(barrier, inc=1, device_id=target, device_id_type=MESH)

    for target in (to_partner, to_left, to_right):
        greet(target)

    @pl.when(z >= 1)
    def _():
        greet(chip_at(-1))

    has_next = z + 1 < chips

    def remote(src, dst, ssem, rsem, target):
        return pltpu.make_async_remote_copy(
            src_ref=src, dst_ref=dst, send_sem=ssem, recv_sem=rsem, device_id=target,
            device_id_type=MESH,
        )

    def onward(h, k):
        piece = pl.ds(k * (quarter // 2), quarter // 2)
        return remote(
            kv.at[h, core, x, piece], kv.at[h + 1, core, x, piece], zs.at[h + 1, k],
            zr.at[h + 1, k], chip_at(1),
        )

    def beside(h, k):
        owner = (x, x, left, right)[k]
        target = (to_right, to_left, to_right, to_left)[k]
        part = kv.at[h, core, owner]
        if k >= 2:
            part = part.at[pl.ds((k - 2) * (quarter // 2), quarter // 2)]
        return remote(part, part, xs.at[h, k], xr_.at[h, k], target)

    def shared(h):
        return [
            remote(
                r.at[h, core], r.at[h, core], ds.at[h, k], dr.at[h, k], to_partner
            )
            for k, r in enumerate((keys_ref, values_ref))
        ]

    step = -math.log(10000.0) / (ROPE // 2)
    frequency = jnp.exp(
        lax.broadcasted_iota(jnp.int32, (ROPE // 2, rows), 0).astype(F32) * step
    )
    position = (sp * rows + lax.broadcasted_iota(jnp.int32, (ROPE // 2, rows), 1)).astype(F32)
    angles = position * frequency
    cosine, sine = jnp.cos(angles), jnp.sin(angles)

    def turned(source):
        a, b = source[: ROPE // 2], source[ROPE // 2 :]
        return jnp.concatenate([a * cosine - b * sine, a * sine + b * cosine], axis=0)

    docs = jnp.broadcast_to(doc_ref[...], (ROPE, rows))
    same_doc = docs == lax.broadcasted_iota(jnp.int32, (ROPE, rows), 0)
    key_tail = jnp.concatenate(
        [turned(rk_ref[...].astype(F32)), same_doc.astype(F32)], axis=0
    ).T.astype(BF16)
    latent = norm_rows(kl_ref[...], kg_ref[...][None, :]).astype(BF16)
    own = jnp.concatenate([latent, key_tail], axis=1)
    kv[0, core] = own.reshape(4, quarter, own.shape[1])
    pl.semaphore_wait(barrier, 3 + has_next.astype(jnp.int32))

    @pl.when(has_next)
    def _():
        onward(0, 0).start()
        onward(0, 1).start()


    def project(h):
        block = kv[h, core].reshape(rows, kv.shape[-1])
        latent = block[:, :latent_width]
        keys_ref[h, core, :, :latent_width] = dot(latent, wk_ref[...]).astype(BF16)
        keys_ref[h, core, :, latent_width:] = block[:, latent_width:]
        values_ref[h, core] = lax.dot_general(
            wv_ref[...], latent, (((0,), (1,)), ((), ())), preferred_element_type=F32
        ).astype(BF16)
        for copy in shared(h):
            copy.start()

    project(0)

    query_normed = norm_rows(ql_ref[...], qg_ref[...][None, :]).astype(BF16)
    nope = lax.dot_general(
        wqn_ref[...], query_normed, (((0,), (1,)), ((), ())), preferred_element_type=F32
    )
    rot = dot_nt(wqr_ref[...], query_normed)
    reject = jnp.where(same_doc, 0.0, FLOOR_SCORE)
    for h in range(heads):
        q_ref[h] = jnp.concatenate(
            [nope[h * NOPE : (h + 1) * NOPE], turned(rot[h * ROPE : (h + 1) * ROPE]), reject],
            axis=0,
        ).astype(BF16)

    def attend(h, blocks, diagonal):
        scores, values = [], []
        for b in blocks:
            keys = keys_ref[h, b]
            tail = keys[:, latent_width:]
            values.append(values_ref[h, b])
            scores.append([
                dot(
                    jnp.concatenate([keys[:, i * NOPE : (i + 1) * NOPE], tail], axis=1), q_ref[i]
                )
                for i in range(heads)
            ])
        if diagonal:
            shape = (rows, rows)
            col = core * rows + lax.broadcasted_iota(jnp.int32, shape, 1)
            row = lax.broadcasted_iota(jnp.int32, shape, 0)
            scores = [
                [jnp.where(row + k * rows <= col, s, FLOOR_SCORE) for s in block]
                for k, block in enumerate(scores)
            ]
        for i in range(heads):
            mine = [block[i] for block in scores]
            highest = functools.reduce(
                jnp.maximum, [jnp.max(s, axis=0, keepdims=True) for s in mine]
            )
            if not diagonal:
                old = m_ref[i]
                highest = jnp.maximum(old, highest)
            weights = [jnp.exp((s - highest) * factor) for s in mine]
            total = sum(jnp.sum(w, axis=0, keepdims=True) for w in weights)
            attended = sum(
                dot(v[i * VDIM : (i + 1) * VDIM], w.astype(BF16)) for v, w in zip(values, weights)
            )
            if not diagonal:
                shrink = jnp.exp((old - highest) * factor)
                total = l_ref[i] * shrink + total
                attended = acc_ref[i] * shrink + attended
            m_ref[i] = highest
            l_ref[i] = total
            acc_ref[i] = attended

    def exists(h):
        return (h >= 1) & (h <= z) & ((h < hops) | ((h == hops) & (core == 1)))

    def goes_on(h):
        more = (h < hops - 1) | ((h == hops - 1) & (core == 1))
        return more & has_next

    def arrive(h):
        @pl.when(exists(h))
        def _():
            for k in range(2):
                onward(h - 1, k).wait_recv()

                @pl.when(goes_on(h))
                def _():
                    onward(h, k).start()

            beside(h, 0).start()
            beside(h, 1).start()

    def pass_on(h):
        @pl.when(exists(h))
        def _():
            beside(h, 0).wait_recv()
            beside(h, 2).start()
            beside(h, 1).wait_recv()
            beside(h, 3).start()

    def share(h):
        @pl.when(exists(h))
        def _():
            beside(h, 2).wait_recv()
            beside(h, 3).wait_recv()
            project(h)

    def use(h):
        @pl.when((h >= 1) & (h < hops) & (h <= z))
        def _():
            for copy in shared(h):
                copy.wait_recv()
            attend(h, (0, 1), False)

    arrive(1)
    for copy in shared(0):
        copy.wait_recv()
    attend(0, (0, 1), True)

    def tick(t, carry):
        arrive(t)
        pass_on(t - 1)
        share(t - 3)
        use(t - 4)
        return carry

    lax.fori_loop(2, hops + 4, tick, 0)

    @pl.when((core == 0) & (hops <= z))
    def _():
        for copy in shared(hops):
            copy.wait_recv()
        attend(hops, (1,), False)

    for i in range(heads):
        out_ref[:, i * VDIM : (i + 1) * VDIM] = (acc_ref[i] / l_ref[i]).T.astype(out_ref.dtype)

    @pl.when(has_next)
    def _():
        onward(0, 0).wait_send()
        onward(0, 1).wait_send()

    for copy in shared(0):
        copy.wait_send()

    def drain(h, carry):
        @pl.when(exists(h))
        def _():
            @pl.when(goes_on(h))
            def _():
                onward(h, 0).wait_send()
                onward(h, 1).wait_send()

            for k in range(4):
                beside(h, k).wait_send()
            for copy in shared(h):
                copy.wait_send()

        return carry

    lax.fori_loop(1, hops + 1, drain, 0)


def attention(
    query_latent, kv_latent, rotary_key, doc_ids, query_gain, kv_gain, w_query_nope, w_query_rot,
    w_key, w_value,
):
    rows = query_latent.shape[0]
    heads = w_key.shape[1] // NOPE
    width = heads * VDIM
    latent_width = kv_latent.shape[1]
    blocks_back = (DOC_MOST + rows - 2) // rows
    hops = (blocks_back + 1) // 2
    assert blocks_back % 2 == 1
    vmem = pl.BlockSpec(memory_space=pltpu.VMEM)
    dma = pltpu.SemaphoreType.DMA
    return pl.pallas_call(
        functools.partial(attention_kernel, (NOPE + ROPE) ** (-0.5), hops),
        out_shape=jax.ShapeDtypeStruct((rows, width), BF16),
        in_specs=[vmem] * 10,
        out_specs=vmem,
        scratch_shapes=[
            pltpu.VMEM((hops + 1, 2, 4, rows // 4, latent_width + 2 * ROPE), BF16),
            pltpu.VMEM((hops + 1, 2, rows, width + 2 * ROPE), BF16),
            pltpu.VMEM((hops + 1, 2, width, rows), BF16),
            pltpu.VMEM((heads, 2 * NOPE, rows), BF16),
            pltpu.VMEM((heads, 1, rows), F32),
            pltpu.VMEM((heads, 1, rows), F32),
            pltpu.VMEM((heads, VDIM, rows), F32),
            dma((hops + 1, 2)),
            dma((hops + 1, 2)),
            dma((hops + 1, 4)),
            dma((hops + 1, 4)),
            dma((hops + 1, 2)),
            dma((hops + 1, 2)),
        ],
        compiler_params=pltpu.CompilerParams(
            collective_id=1, has_side_effects=True, vmem_limit_bytes=56 * 1024 * 1024
        ),
    )(
        query_latent, kv_latent, rotary_key.T, doc_ids[None, :],
        query_gain, kv_gain, w_query_nope, w_query_rot.T, w_key, w_value,
    )


COLS = 512
SPAN = 2


def offsets_of(chips):
    half, quarter = chips // 2, chips // 4
    offsets = [0, 1, -2, 3]
    for m in range(half - 1, quarter, -1):
        offsets += [m, -m]
    offsets += [half, -quarter]
    for m in range(quarter, 3, -1):
        offsets += [m, 1 - m]
    return offsets + [2, -1]


def mixer_kernel(
    chips,
    att_ref, res_ref, gain_ref, routes_ref, group_ref, logits_ref, wout_hbm, wg_hbm, wu_hbm, wd_hbm,
    out_ref,
    wout_ref, wg_ref, wu_ref, wd_ref, wgt_ref, wut_ref, part, relay_l, relay_r, sum_r, sum_l, from_l, from_r, mixed,
    meta, tok, sendb, rec, back_t, back_rl, back_rr, back_sr, back_sl, back_fl, back_fr, zb, gb,
    gb2, way, way_back, outb,
    wsem, wosem, osem, ws, wr, pair_s, pair_r, hs, hr, ps, pr, zs, zr, xs, xr_, bs, br, gs, gr,
):
    sp = lax.axis_index("sp")
    x = lax.axis_index("tp")
    core = lax.rem(sp, 2)
    z = lax.div(sp, 2)
    partner = sp + 1 - 2 * core
    right, left, across = lax.rem(x + 1, 4), lax.rem(x + 3, 4), lax.rem(x + 2, 4)
    to_right, to_left, to_partner = {"tp": right}, {"tp": left}, {"sp": partner}
    offsets = offsets_of(chips)
    n_chunks = chips // SPAN
    rows, width = res_ref.shape
    half = width // 2

    def on_ring(offset):
        return {"sp": lax.rem(z + offset + chips, chips) * 2 + core}

    barrier = pltpu.get_barrier_semaphore()
    for target in [to_partner, to_left, to_right] + [on_ring(o) for o in offsets[1:]]:
        pl.semaphore_signal(barrier, inc=1, device_id=target, device_id_type=MESH)

    tiles = width // COLS

    def cols_of(t):
        return pl.ds(pl.multiple_of(t * COLS, COLS), COLS)

    def w_load(t):
        return pltpu.make_async_copy(
            wout_hbm.at[:, cols_of(t)], wout_ref.at[:, cols_of(t)], wosem.at[t]
        )

    for t in range(tiles):
        w_load(t).start()
    loads = [
        pltpu.make_async_copy(wg_hbm, wg_ref, wsem.at[0]),
        pltpu.make_async_copy(wu_hbm, wu_ref, wsem.at[1]),
        pltpu.make_async_copy(wd_hbm, wd_ref, wsem.at[2]),
    ]

    def remote(src, dst, ssem, rsem, target):
        return pltpu.make_async_remote_copy(
            src_ref=src, dst_ref=dst, send_sem=ssem, recv_sem=rsem, device_id=target,
            device_id_type=MESH,
        )

    def project(t, carry):
        w_load(t).wait()
        value = dot(att_ref[...], wout_ref[:, cols_of(t)])
        part[:, :, cols_of(t)] = value.reshape(4, rows, COLS).astype(BF16)
        return carry

    sends = []

    def start(copy):
        copy.start()
        sends.append(copy)
        return copy

    lo, hi = pl.ds(0, half), pl.ds(half, half)
    lax.fori_loop(0, tiles // 2, project, 0)
    pl.semaphore_wait(barrier, 3 + len(offsets) - 1)
    c_a = start(remote(part.at[across, :, lo], relay_l, ps.at[0], pr.at[0], to_right))
    c_d = start(remote(part.at[left, :, lo], from_r.at[:, lo], ps.at[1], pr.at[1], to_left))
    lax.fori_loop(tiles // 2, tiles, project, 0)
    for load in loads:
        load.start()
    c_b = start(remote(part.at[across, :, hi], relay_r, ps.at[2], pr.at[2], to_left))
    c_c = start(remote(part.at[right, :, hi], from_l.at[:, hi], ps.at[3], pr.at[3], to_right))
    routes = routes_ref[...]
    expert = lax.broadcasted_iota(jnp.int32, (2 * chips, rows), 0)
    goes = [routes[k : k + 1] == expert for k in range(2)]
    earlier = (
        lax.broadcasted_iota(jnp.int32, (rows, rows), 0)
        < lax.broadcasted_iota(jnp.int32, (rows, rows), 1)
    )
    before = dot(
        (goes[0] | goes[1]).astype(F32).astype(BF16), earlier.astype(F32).astype(BF16)
    )
    distance = lax.rem(lax.div(routes, 2) - z + chips, chips)
    place = jnp.zeros_like(routes)
    for p, offset in enumerate(offsets):
        place = jnp.where(distance == offset % chips, p, place)
    spot = (lax.rem(routes, 2) * (8 * chips) + place * 8 + core * 4).astype(F32)
    ranks = [jnp.sum(jnp.where(g, before, 0.0), axis=0, keepdims=True) for g in goes]
    logits = logits_ref[...]
    top = jnp.maximum(logits[0:1], logits[1:2])
    powers = [jnp.exp(logits[k : k + 1] - top) for k in range(2)]
    share = group_ref[...][None, :] / (powers[0] + powers[1])
    table = [spot[k : k + 1] + ranks[k] for k in range(2)] + [p * share for p in powers]
    table.append(jnp.zeros((meta.shape[2] - 4, rows), F32))
    meta[core] = jnp.concatenate(table, axis=0).T

    m_x = start(remote(meta.at[core], meta.at[core], pair_s.at[0], pair_r.at[0], to_partner))
    c_a.wait_recv()
    sum_r[...] = (part[right, :, :half].astype(F32) + relay_l[...].astype(F32)).astype(BF16)
    c_e = start(remote(sum_r, from_l.at[:, lo], ps.at[4], pr.at[4], to_right))
    c_b.wait_recv()
    sum_l[...] = (part[left, :, half:].astype(F32) + relay_r[...].astype(F32)).astype(BF16)
    c_f = start(remote(sum_l, from_r.at[:, hi], ps.at[5], pr.at[5], to_left))
    for load in loads:
        load.wait()

    def turn(t, carry):
        wgt_ref[cols_of(t), :] = wg_ref[:, cols_of(t)].T
        wut_ref[cols_of(t), :] = wu_ref[:, cols_of(t)].T
        return carry

    lax.fori_loop(0, tiles, turn, 0)
    for copy in (c_d, c_c, c_e, c_f):
        copy.wait_recv()

    after = (
        res_ref[...].astype(F32)
        + (part[x].astype(F32) + from_l[...].astype(F32) + from_r[...].astype(F32))
    ).astype(BF16)
    mixed[...] = after
    tok[core] = norm_rows(after, gain_ref[...][None, :]).astype(BF16)
    t_x = start(remote(tok.at[core], tok.at[core], pair_s.at[1], pair_r.at[1], to_partner))
    m_x.wait_recv()
    keys = meta[...].reshape(2 * rows, meta.shape[2])
    slots = 8 * chips
    wanted = (lax.broadcasted_iota(jnp.int32, (2 * rows, slots), 1) + core * slots).astype(F32)
    first = keys[:, 0:1] == wanted
    second = keys[:, 1:2] == wanted
    choose = (first | second).astype(F32).astype(BF16)
    t_x.wait_recv()

    def select(t, carry):
        source = tok[:, :, cols_of(t)].reshape(2 * rows, COLS)
        picked = lax.dot_general(
            choose, source, (((0,), (0,)), ((), ())), preferred_element_type=F32
        )
        sendb[:, :, cols_of(t)] = picked.reshape(chips, 8, COLS).astype(BF16)
        return carry

    opposite = offsets.index(chips // 2)
    quarter = chips // 4

    def both_ways(block, buffers, first, ssems, rsems):
        return [
            start(
                remote(
                    block.at[:, cols], buffers.at[k], ssems.at[first + k], rsems.at[first + k],
                    on_ring(side * quarter),
                )
            )
            for k, (cols, side) in enumerate(((lo, 1), (hi, -1)))
        ]

    def hand_on(arriving, buffers, block):
        base = 0 if buffers is way else 4
        for k, (cols, side) in enumerate(((lo, 1), (hi, -1))):
            arriving[k].wait_recv()
            arriving.append(
                start(
                    remote(
                        buffers.at[k], block.at[:, cols], ws.at[base + 2 + k],
                        wr.at[base + 2 + k], on_ring(side * quarter),
                    )
                )
            )

    def arrived_in_full(copies):
        for copy in copies[2:] if isinstance(copies, list) else [copies]:
            copy.wait_recv()

    lax.fori_loop(0, tiles, select, 0)
    z_out = [None]
    z_out += [None] * (chips - 1)

    def send_blocks(positions):
        for p in positions:
            z_out[p] = start(
                remote(sendb.at[p], rec.at[x, p], zs.at[p], zr.at[p], on_ring(offsets[p]))
            )

    send_blocks(range(1, SPAN * 2))
    z_out[opposite] = both_ways(sendb.at[opposite], way, 0, ws, wr)
    send_blocks(range(SPAN * 2, opposite))
    rec[x, 0] = sendb[0]

    fwd = [None] * n_chunks

    def spread(q):
        for p in range(q * SPAN, (q + 1) * SPAN):
            if p:
                arrived_in_full(z_out[p])
        whole = pl.ds(q * SPAN, SPAN)
        fwd[q] = [
            start(remote(rec.at[x, whole], rec.at[x, whole], xs.at[q, 0], xr_.at[q, 0], to_right)),
            start(remote(rec.at[x, whole], rec.at[x, whole], xs.at[q, 1], xr_.at[q, 1], to_left)),
        ]

    relays = [None] * n_chunks

    def relay(q):
        a = pl.ds(q * SPAN, SPAN // 2)
        b = pl.ds(q * SPAN + SPAN // 2, SPAN // 2)
        fwd[q][0].wait_recv()
        one = start(remote(rec.at[left, a], rec.at[left, a], xs.at[q, 2], xr_.at[q, 2], to_right))
        fwd[q][1].wait_recv()
        two = start(remote(rec.at[right, b], rec.at[right, b], xs.at[q, 3], xr_.at[q, 3], to_left))
        relays[q] = [one, two]

    backs = [None] * n_chunks
    lo2, hi2 = pl.ds(0, SPAN // 2), pl.ds(SPAN // 2, SPAN // 2)

    def experts(q):
        for copy in relays[q]:
            copy.wait_recv()
        many = 4 * SPAN * 8
        arrived = rec[:, q * SPAN : (q + 1) * SPAN].reshape(many, width)
        gate = dot(arrived, wgt_ref[...])
        up = dot(arrived, wut_ref[...])
        hidden = (gate / (1.0 + jnp.exp(-gate)) * up).astype(BF16)

        def down(t, carry):
            value = dot(hidden, wd_ref[:, cols_of(t)])
            back_t[q, :, :, :, cols_of(t)] = value.reshape(4, SPAN, 8, COLS).astype(BF16)
            return carry

        lax.fori_loop(0, tiles, down, 0)
        own = back_t.at[q]
        backs[q] = [
            start(remote(own.at[across, lo2], back_rl.at[q], bs.at[q, 0], br.at[q, 0], to_right)),
            start(remote(own.at[across, hi2], back_rr.at[q], bs.at[q, 1], br.at[q, 1], to_left)),
            start(remote(own.at[right, hi2], back_fl.at[q, hi2], bs.at[q, 2], br.at[q, 2], to_right)),
            start(remote(own.at[left, lo2], back_fr.at[q, lo2], bs.at[q, 3], br.at[q, 3], to_left)),
        ]

    def add_relayed(q):
        backs[q][0].wait_recv()
        back_sr[q] = (
            back_t[q, right, : SPAN // 2].astype(F32) + back_rl[q].astype(F32)
        ).astype(BF16)
        backs[q].append(
            start(remote(back_sr.at[q], back_fl.at[q, lo2], bs.at[q, 4], br.at[q, 4], to_right))
        )
        backs[q][1].wait_recv()
        back_sl[q] = (
            back_t[q, left, SPAN // 2 :].astype(F32) + back_rr[q].astype(F32)
        ).astype(BF16)
        backs[q].append(
            start(remote(back_sl.at[q], back_fr.at[q, hi2], bs.at[q, 5], br.at[q, 5], to_left))
        )

    g_out = [None] * chips

    def give_back(q):
        for copy in backs[q][2:]:
            copy.wait_recv()
        zb[q] = (
            back_t[q, x].astype(F32) + back_fl[q].astype(F32) + back_fr[q].astype(F32)
        ).astype(BF16)
        for k in range(SPAN):
            p = q * SPAN + k
            if p == opposite:
                g_out[p] = both_ways(zb.at[q, k], way_back, 4, ws, wr)
            elif p:
                g_out[p] = start(
                    remote(zb.at[q, k], gb.at[p], gs.at[p], gr.at[p], on_ring(-offsets[p]))
                )
            else:
                gb[0] = zb[0, 0]

    stages = ((give_back, 4), (add_relayed, 3), (experts, 2), (relay, 1), (spread, 0))
    opposite_chunk = opposite // SPAN
    for tick in range(n_chunks + 4):
        if tick == 2:
            hand_on(z_out[opposite], way, rec.at[x, opposite])
            send_blocks(range(opposite + 1, chips))
        if tick == opposite_chunk + 5:
            hand_on(g_out[opposite], way_back, gb.at[opposite])
        for stage, lag in stages:
            if 0 <= tick - lag < n_chunks:
                stage(tick - lag)

    across_cores = []
    for p in range(chips):
        if p:
            arrived_in_full(g_out[p])
        across_cores.append(start(remote(gb.at[p], gb2.at[p], hs.at[p], hr.at[p], to_partner)))
    mine = meta[core]

    def weigh(parity):
        here = (
            lax.broadcasted_iota(jnp.int32, (rows, slots), 1) + parity * slots
        ).astype(F32)
        weight = jnp.where(mine[:, 0:1] == here, mine[:, 2:3], 0.0)
        weight = weight + jnp.where(mine[:, 1:2] == here, mine[:, 3:4], 0.0)
        high = weight.astype(BF16)
        return high, (weight - high.astype(F32)).astype(BF16)

    weights = [weigh(core), weigh(1 - core)]
    for copy in across_cores:
        copy.wait_recv()

    def combine(t, carry):
        routed = 0.0
        for (high, low), blocks in zip(weights, (gb, gb2)):
            returned = blocks[:, :, cols_of(t)].reshape(slots, COLS)
            routed = routed + (dot(high, returned) + dot(low, returned))
        outb[:, cols_of(t)] = (mixed[:, cols_of(t)].astype(F32) + routed).astype(outb.dtype)
        put_out(t).start()
        return carry

    def put_out(t):
        return pltpu.make_async_copy(
            outb.at[:, cols_of(t)], out_ref.at[:, cols_of(t)], osem.at[t]
        )

    lax.fori_loop(0, tiles, combine, 0)
    for t in range(tiles):
        put_out(t).wait()
    for copy in sends:
        copy.wait_send()


def mixer(
    attended, w_out, residual, gain, routes, group_weight, logits, w_gate, w_up, w_down, chips
):
    rows, width = residual.shape
    n_chunks = chips // SPAN
    vmem = pl.BlockSpec(memory_space=pltpu.VMEM)
    hbm = pl.BlockSpec(memory_space=pl.ANY)
    half = width // 2
    dma = pltpu.SemaphoreType.DMA
    chunk = (n_chunks, SPAN, 8, width)
    half_chunk = (n_chunks, SPAN // 2, 8, width)
    return pl.pallas_call(
        functools.partial(mixer_kernel, chips),
        out_shape=jax.ShapeDtypeStruct((rows, width), BF16),
        in_specs=[vmem] * 6 + [hbm] * 4,
        out_specs=hbm,
        scratch_shapes=[
            pltpu.VMEM(w_out.shape, BF16),
            pltpu.VMEM(w_gate.shape, BF16),
            pltpu.VMEM(w_up.shape, BF16),
            pltpu.VMEM(w_down.shape, BF16),
            pltpu.VMEM(w_gate.shape[::-1], BF16),
            pltpu.VMEM(w_up.shape[::-1], BF16),
            pltpu.VMEM((4, rows, width), BF16),
            pltpu.VMEM((rows, half), BF16),
            pltpu.VMEM((rows, half), BF16),
            pltpu.VMEM((rows, half), BF16),
            pltpu.VMEM((rows, half), BF16),
            pltpu.VMEM((rows, width), BF16),
            pltpu.VMEM((rows, width), BF16),
            pltpu.VMEM((rows, width), BF16),
            pltpu.VMEM((2, rows, 128), F32),
            pltpu.VMEM((2, rows, width), BF16),
            pltpu.VMEM((chips, 8, width), BF16),
            pltpu.VMEM((4, chips, 8, width), BF16),
            pltpu.VMEM((n_chunks, 4, SPAN, 8, width), BF16),
            pltpu.VMEM(half_chunk, BF16),
            pltpu.VMEM(half_chunk, BF16),
            pltpu.VMEM(half_chunk, BF16),
            pltpu.VMEM(half_chunk, BF16),
            pltpu.VMEM(chunk, BF16),
            pltpu.VMEM(chunk, BF16),
            pltpu.VMEM(chunk, BF16),
            pltpu.VMEM((chips, 8, width), BF16),
            pltpu.VMEM((chips, 8, width), BF16),
            pltpu.VMEM((2, 8, half), BF16),
            pltpu.VMEM((2, 8, half), BF16),
            pltpu.VMEM((rows, width), BF16),
            dma((3,)),
            dma((width // COLS,)),
            dma((width // COLS,)),
            dma((8,)),
            dma((8,)),
            dma((2,)),
            dma((2,)),
            dma((chips,)),
            dma((chips,)),
            dma((6,)),
            dma((6,)),
            dma((chips,)),
            dma((chips,)),
            dma((n_chunks, 4)),
            dma((n_chunks, 4)),
            dma((n_chunks, 6)),
            dma((n_chunks, 6)),
            dma((chips,)),
            dma((chips,)),
        ],
        compiler_params=pltpu.CompilerParams(
            collective_id=0, has_side_effects=True, vmem_limit_bytes=56 * 1024 * 1024
        ),
    )(attended, residual, gain, routes, group_weight, logits, w_out, w_gate, w_up, w_down)


def on_device(
    residual,
    query_latent,
    kv_latent,
    rotary_key,
    doc_ids,
    query_gain,
    kv_gain,
    w_query_nope,
    w_query_rot,
    w_key_nope,
    w_value,
    w_out,
    ffn_gain,
    w_gate,
    w_up,
    w_down,
    routes,
    group_weight,
    member_logits,
):
    chips = lax.axis_size("sp") // 2
    attended = attention(
        query_latent, kv_latent, rotary_key, doc_ids, query_gain, kv_gain, w_query_nope,
        w_query_rot, w_key_nope, w_value,
    )
    return mixer(
        attended, w_out, residual, ffn_gain, routes.T, group_weight, member_logits.T,
        w_gate[0].T, w_up[0].T, w_down[0], chips,
    )


def solution(mesh):
    return jax.shard_map(
        on_device,
        mesh=mesh,
        in_specs=(
            P(("grp", "sp", "tp"), None),
            P(("grp", "sp"), None),
            P(("grp", "sp"), None),
            P(("grp", "sp"), None),
            P(("grp", "sp")),
            P(),
            P(),
            P(None, "tp"),
            P(None, "tp"),
            P(None, "tp"),
            P(None, "tp"),
            P("tp", None),
            P(),
            P("sp", None, "tp"),
            P("sp", None, "tp"),
            P("sp", "tp", None),
            P(("grp", "sp", "tp"), None),
            P(("grp", "sp", "tp")),
            P(("grp", "sp", "tp"), None),
        ),
        out_specs=P(("grp", "sp", "tp"), None),
        check_vma=False,
    )
```
